32 devices in a mesh: sp: 8 (over z, y), tp: 4 (over x, core).
Axes of the slice: x: 2, y: 2, z: 4, core: 2. Of those that a mesh axis runs over, the one named last changes fastest.
Arguments:
- latent: bfloat16 [3072, 2048], P(('sp', 'tp')), may hold values from -6 to 6
- context: bfloat16 [512, 2048], P('sp'), may hold values from -6 to 6
- cond_latent: float32 [2048], replicated, may hold values from -6 to 6
- cond_context: float32 [2048], replicated, may hold values from -12 to 12
- shift_weight: bfloat16 [2048, 2048], P('sp', 'tp'), may hold values from -0.125 to 0.125
- scale_weight: bfloat16 [2048, 2048], P('sp', 'tp'), may hold values from -0.125 to 0.125
- gate_weight: bfloat16 [2048, 2048], P('sp', 'tp'), may hold values from -0.125 to 0.125
- query_weight: bfloat16 [2, 2048, 1024], P(None, None, 'tp'), may hold values from -1.3258252 to 1.3258252
- key_weight: bfloat16 [2, 2048, 1024], P(None, None, 'tp'), may hold values from -1.3258252 to 1.3258252
- value_weight: bfloat16 [2048, 2048], P(None, 'tp'), may hold values from -0.125 to 0.125
- out_weight: bfloat16 [2048, 2048], P('tp'), may hold values from -0.125 to 0.125
- lambda_heads: float32 [16], P('tp'), may hold values from 0.3 to 0.8
- out_gain: float32 [2048], P('tp'), may hold values from 0.1 to 1.9
Outputs:
- result: bfloat16 [3072, 2048], P(('sp', 'tp'))
The draws below stay inside these ranges and needn't reach their ends.
All inputs are finite; a program needn't handle non-finite values.
Results may differ from the reference program's by a relative error of at most 0.02.
The reference program's roundings to bfloat16 on the way count: a program that leaves them out, or rounds other values in their place, can miss the bound.
Values may be sent and summed in bfloat16 or wider, within the bound.
No kernel may reach another device: no remote copies, remote signals or barrier semaphores. Data moves between devices by JAX's collectives and lax.ppermute only.
A program may use at most 128 MiB of HBM per device.

```python
import math
import jax
import jax.numpy as jnp
from jax import lax

D = 2048
HEADS = 16
HEAD_DIM = 64
GRID_W = 64
CTX = 512
VALUE_DIM = 128
TOKENS = 3072
N_TP = 4


def projection(key, salt_value):
    entries = jax.random.truncated_normal(jax.random.fold_in(key, salt_value), -6.0, 6.0, (2, D, HEADS, HEAD_DIM), jnp.float32)
    scaled = entries * D ** (-0.5)
    return scaled.reshape(2, D, HEADS * HEAD_DIM).astype(jnp.bfloat16)


def draw_query_weight(key, part):
    return projection(key, 11)


def draw_key_weight(key, part):
    return projection(key, 23)


def level_of(own_key, extent, shards, low, top_value):
    gain = 1.0
    for dim, shards_of in shards:
        steps = jax.random.uniform(jax.random.fold_in(jax.random.fold_in(own_key, 6), dim), (shards_of,), jnp.float32, low / len(shards), top_value / len(shards))
        gain = gain * jnp.repeat(jnp.exp(steps), extent[dim] // shards_of).reshape((-1,) + (1,) * (len(extent) - 1 - dim))
    return gain


def gaussian(stream_key, extent, spread, reach, cuts=(), held_as=jnp.bfloat16):
    values = spread * jax.random.normal(stream_key, extent, jnp.float32)
    if cuts:
        values = values * level_of(stream_key, extent, cuts, -0.22, 0.18)
    return jnp.clip(values, -reach, reach).astype(held_as)


def setup_inputs(seed: int = 0) -> dict:
    streams_of = jax.random.split(jax.random.key(seed), 14)
    latent = gaussian(streams_of[0], (TOKENS, D), 1.0, 6.0, ((0, 32),))
    context = gaussian(streams_of[1], (CTX, D), 1.0, 6.0, ((0, 8),))
    cond_latent = gaussian(streams_of[2], (D,), 1.0, 6.0, (), jnp.float32)
    cond_context = gaussian(streams_of[3], (D,), 2.0, 12.0, (), jnp.float32)
    shift_weight = gaussian(streams_of[4], (D, D), D ** -0.5, 0.125, ((0, 8), (1, 4)))
    scale_weight = gaussian(streams_of[5], (D, D), D ** -0.5, 0.125, ((0, 8), (1, 4)))
    gate_weight = gaussian(streams_of[6], (D, D), D ** -0.5, 0.125, ((0, 8), (1, 4)))
    query_weight = draw_query_weight(jax.random.fold_in(streams_of[13], 71), 0)
    key_weight = draw_key_weight(jax.random.fold_in(streams_of[13], 71), 0)
    value_weight = gaussian(streams_of[9], (D, HEADS * VALUE_DIM), D ** -0.5, 0.125, ((1, 4),))
    out_weight = gaussian(streams_of[10], (HEADS * VALUE_DIM, D), (HEADS * VALUE_DIM) ** -0.5, 0.125, ((0, 4),))
    lambda_heads = jnp.clip(0.3 + 0.5 * jax.random.uniform(streams_of[11], (HEADS,), jnp.float32) ** level_of(streams_of[11], (HEADS,), ((0, 4),), -0.2, 0.2), 0.3, 0.8)
    out_gain = jnp.clip(1.0 + 0.18 * jax.random.normal(streams_of[12], (HEADS * VALUE_DIM,), jnp.float32), 0.1, 1.9)
    return dict(latent=latent, context=context, cond_latent=cond_latent, cond_context=cond_context, shift_weight=shift_weight, scale_weight=scale_weight, gate_weight=gate_weight, query_weight=query_weight, key_weight=key_weight, value_weight=value_weight, out_weight=out_weight, lambda_heads=lambda_heads, out_gain=out_gain)


norm_eps = 1e-06
rope_theta = 10000.0

def rms_scale(matrix):
    return matrix * lax.rsqrt(lax.optimization_barrier(jnp.mean(matrix * matrix, axis=-1, keepdims=True)) + norm_eps)

def modulated(activations, shift, scale):
    return (rms_scale(activations.astype(jnp.float32)) * (1.0 + scale) + shift).astype(jnp.bfloat16)

def rotate(vectors, positions, grid_width):
    quarter = vectors.shape[-1] // 4
    inverse = rope_theta ** (-jnp.arange(quarter, dtype=jnp.float32) / quarter)
    grid_row = (positions // grid_width).astype(jnp.float32)
    grid_col = (positions % grid_width).astype(jnp.float32)
    angles = jnp.concatenate([grid_row[:, None] * inverse, grid_col[:, None] * inverse], axis=-1)
    cos_table = jnp.cos(angles)[:, None, :]
    sin_table = jnp.sin(angles)[:, None, :]
    former = vectors[..., :2 * quarter]
    latter = vectors[..., 2 * quarter:]
    return jnp.concatenate([former * cos_table - latter * sin_table, latter * cos_table + former * sin_table], axis=-1)

def reference(latent, context, cond_latent, cond_context, shift_weight, scale_weight, gate_weight, query_weight, key_weight, value_weight, out_weight, lambda_heads, out_gain):
    conditions = jax.nn.silu(jnp.stack([cond_latent, cond_context])).astype(jnp.bfloat16)
    shifts = jnp.dot(conditions, shift_weight, preferred_element_type=jnp.float32)
    scales = jnp.dot(conditions, scale_weight, preferred_element_type=jnp.float32)
    gate_vector = jnp.dot(conditions[:1], gate_weight, preferred_element_type=jnp.float32)[0]
    hidden = modulated(latent, shifts[0], scales[0])
    context_hidden = modulated(context, shifts[1], scales[1])
    positions = jnp.arange(TOKENS, dtype=jnp.int32)

    def latent_heads(weight):
        product = jnp.dot(hidden, weight, preferred_element_type=jnp.float32).reshape(TOKENS, HEADS, HEAD_DIM)
        return rotate(product, positions, GRID_W).astype(jnp.bfloat16)

    def context_heads(weight):
        product = jnp.dot(context_hidden, weight, preferred_element_type=jnp.float32)
        return product.reshape(CTX, HEADS, HEAD_DIM).astype(jnp.bfloat16)
    queries = jnp.stack([latent_heads(query_weight[0]), latent_heads(query_weight[1])])
    key_rows = jnp.stack([jnp.concatenate([context_heads(key_weight[which_map]), latent_heads(key_weight[which_map])], axis=0) for which_map in (0, 1)])
    value_rows = jnp.concatenate([jnp.dot(context_hidden, value_weight, preferred_element_type=jnp.float32).astype(jnp.bfloat16), jnp.dot(hidden, value_weight, preferred_element_type=jnp.float32).astype(jnp.bfloat16)], axis=0)
    queries, key_rows, value_rows = lax.optimization_barrier((queries, key_rows, value_rows))
    queries = queries.transpose(2, 0, 1, 3)
    key_rows = key_rows.transpose(2, 0, 1, 3)
    value_rows = value_rows.reshape(CTX + TOKENS, HEADS, VALUE_DIM).transpose(1, 0, 2)
    query_block = math.gcd(TOKENS, 512)

    def one_head(operands):
        head_queries, head_keys, head_values, head_lambda = operands
        key_float = head_keys.astype(jnp.float32)
        value_float = head_values.astype(jnp.float32)
        blocks = head_queries.reshape(2, TOKENS // query_block, query_block, HEAD_DIM).transpose(1, 0, 2, 3)

        def one_block(block_queries):
            scores = jnp.einsum('mqd,mkd->mqk', block_queries.astype(jnp.float32), key_float) * HEAD_DIM ** (-0.5)
            weights = jnp.exp(scores - lax.optimization_barrier(jnp.max(scores, axis=-1, keepdims=True)))
            totals = lax.optimization_barrier(jnp.sum(weights, axis=-1, keepdims=True))
            rounded = lax.optimization_barrier(weights.astype(jnp.bfloat16)).astype(jnp.float32)
            numerator = jnp.einsum('mqk,ke->mqe', rounded, value_float)
            return numerator[0] / totals[0] - head_lambda * (numerator[1] / totals[1])
        return lax.map(one_block, blocks).reshape(TOKENS, VALUE_DIM)
    mixed = lax.map(one_head, (queries, key_rows, value_rows, lambda_heads))
    normed = rms_scale(mixed) * out_gain.reshape(HEADS, 1, VALUE_DIM)
    heads_out = normed.transpose(1, 0, 2).reshape(TOKENS, HEADS * VALUE_DIM).astype(jnp.bfloat16)
    group_width = HEADS // N_TP * VALUE_DIM
    summed = jnp.zeros((TOKENS, D), jnp.float32)
    for group_index in range(N_TP):
        lower = group_index * group_width
        group_term = jnp.dot(heads_out[:, lower:lower + group_width], out_weight[lower:lower + group_width], preferred_element_type=jnp.float32)
        summed = summed + lax.optimization_barrier(group_term.astype(jnp.bfloat16)).astype(jnp.float32)
    return (latent.astype(jnp.float32) + gate_vector * summed).astype(jnp.bfloat16)
```

```python
import functools
import math

import jax
import jax.numpy as jnp
from jax import lax
from jax.experimental import pallas as pl
from jax.experimental.pallas import tpu as pltpu
from jax.sharding import PartitionSpec as P


HEAD_DIM = 64
GRID_W = 64
VALUE_DIM = 128
LANES = 128

norm_eps = 1e-06
rope_theta = 10000.0
block_limit = 1024
query_block = 256


def rms_scale(matrix):
    return matrix * lax.rsqrt(jnp.mean(matrix * matrix, axis=-1, keepdims=True) + norm_eps)


def modulated(activations, shift, scale):
    return (rms_scale(activations.astype(jnp.float32)) * (1.0 + scale) + shift).astype(jnp.bfloat16)


def rope_tables(positions, grid_width, head_dim):
    quarter = head_dim // 4
    inverse = rope_theta ** (-jnp.arange(quarter, dtype=jnp.float32) / quarter)
    grid_row = (positions // grid_width).astype(jnp.float32)
    grid_col = (positions % grid_width).astype(jnp.float32)
    angles = jnp.concatenate([grid_row[:, None] * inverse, grid_col[:, None] * inverse], axis=-1)
    return jnp.cos(angles), jnp.sin(angles)


def rotate(vectors, positions, grid_width):
    quarter = vectors.shape[-1] // 4
    cos_table, sin_table = rope_tables(positions, grid_width, vectors.shape[-1])
    cos_table = cos_table[:, None, :]
    sin_table = sin_table[:, None, :]
    former = vectors[..., : 2 * quarter]
    latter = vectors[..., 2 * quarter :]
    return jnp.concatenate(
        [former * cos_table - latter * sin_table, latter * cos_table + former * sin_table], axis=-1
    )


def absorb(carry_state, key_block, value_block, queries, head_count):
    maxima, totals, numerator = carry_state
    row_count = key_block.shape[0]
    scores = jnp.einsum(
        "mhqd,kmhd->mhqk",
        queries,
        key_block.reshape(row_count, 2, head_count, HEAD_DIM),
        preferred_element_type=jnp.float32,
    ) * HEAD_DIM ** (-0.5)
    new_maxima = jnp.maximum(maxima, jnp.max(scores, axis=-1))
    rescale = jnp.exp(maxima - new_maxima)
    weights = jnp.exp(scores - new_maxima[..., None])
    totals = totals * rescale + jnp.sum(weights, axis=-1)
    numerator = numerator * rescale[..., None] + jnp.einsum(
        "mhqk,khe->mhqe",
        weights.astype(jnp.bfloat16),
        value_block.reshape(row_count, head_count, VALUE_DIM),
        preferred_element_type=jnp.float32,
    )
    return (new_maxima, totals, numerator)


def absorb_all(carry_state, key_rows, value_rows, queries, head_count, shard_len):
    total_rows = key_rows.shape[0]
    shards = total_rows // shard_len
    shard_group = max(
        [
            candidate
            for candidate in range(1, shards + 1)
            if shards % candidate == 0 and candidate * shard_len <= block_limit
        ]
        + [1]
    )
    block_rows = shard_group * shard_len

    def absorb_block(block_index, inner_state):
        key_block = lax.dynamic_slice_in_dim(key_rows, block_index * block_rows, block_rows, 0)
        value_block = lax.dynamic_slice_in_dim(value_rows, block_index * block_rows, block_rows, 0)
        return absorb(inner_state, key_block, value_block, queries, head_count)

    return lax.fori_loop(0, total_rows // block_rows, absorb_block, carry_state)


def local_general(
    latent,
    context,
    cond_latent,
    cond_context,
    shift_weight,
    scale_weight,
    gate_weight,
    query_weight,
    key_weight,
    value_weight,
    out_weight,
    lambda_heads,
    out_gain,
):
    mod_rows = shift_weight.shape[0]
    conditions = jnp.stack([cond_latent, cond_context])
    conditions = jax.nn.silu(
        lax.dynamic_slice_in_dim(conditions, lax.axis_index("sp") * mod_rows, mod_rows, 1)
    )
    conditions = conditions.astype(jnp.bfloat16)
    partial_value = jnp.concatenate(
        [
            jnp.dot(conditions, shift_weight, preferred_element_type=jnp.float32),
            jnp.dot(conditions, scale_weight, preferred_element_type=jnp.float32),
            jnp.dot(conditions[:1], gate_weight, preferred_element_type=jnp.float32),
        ],
        axis=0,
    )
    summed_mod = lax.psum(partial_value, "sp")
    whole_mod = lax.all_gather(summed_mod, "tp", axis=1, tiled=True)
    hidden = modulated(latent, whole_mod[0], whole_mod[2])
    context_hidden = modulated(context, whole_mod[1], whole_mod[3])
    head_count = lambda_heads.shape[0]
    own_rows = latent.shape[0]
    tok_rows = own_rows * lax.axis_size("tp")
    row_offset = lax.axis_index("sp") * tok_rows
    piece_rows = lax.all_gather(hidden, "tp", axis=0, tiled=True)
    row_count = piece_rows.shape[0]
    positions = row_offset + jnp.arange(row_count, dtype=jnp.int32)

    def rotated(weight):
        product = jnp.concatenate(
            [
                jnp.dot(piece_rows, weight[0], preferred_element_type=jnp.float32),
                jnp.dot(piece_rows, weight[1], preferred_element_type=jnp.float32),
            ],
            axis=-1,
        )
        turned = rotate(product.reshape(row_count, 2 * head_count, HEAD_DIM), positions, GRID_W)
        return turned.reshape(row_count, 2 * head_count * HEAD_DIM).astype(jnp.bfloat16)

    values = jnp.dot(piece_rows, value_weight, preferred_element_type=jnp.float32).astype(
        jnp.bfloat16
    )
    key_width = 2 * head_count * HEAD_DIM
    queries = rotated(query_weight).reshape(tok_rows, 2, head_count, HEAD_DIM).transpose(1, 2, 0, 3)
    latent_keys = rotated(key_weight)
    context_keys = jnp.concatenate(
        [
            jnp.dot(context_hidden, key_weight[0], preferred_element_type=jnp.float32),
            jnp.dot(context_hidden, key_weight[1], preferred_element_type=jnp.float32),
        ],
        axis=-1,
    ).astype(jnp.bfloat16)
    context_values = jnp.dot(
        context_hidden, value_weight, preferred_element_type=jnp.float32
    ).astype(jnp.bfloat16)
    state = (
        jnp.full((2, head_count, tok_rows), -jnp.inf, jnp.float32),
        jnp.zeros((2, head_count, tok_rows), jnp.float32),
        jnp.zeros((2, head_count, tok_rows, VALUE_DIM), jnp.float32),
    )
    context_dev = context_keys.shape[0]
    shard_len = tok_rows + context_dev
    value_width = context_values.shape[1]
    context_total = context_dev * lax.axis_size("sp")
    whole_keys = lax.all_gather(jnp.concatenate([latent_keys, context_keys], axis=0), "sp", axis=0, tiled=True)
    whole_values = lax.all_gather(jnp.concatenate([values, context_values], axis=0), "sp", axis=0, tiled=True)
    shard_count = whole_keys.shape[0] // shard_len
    key_parts = whole_keys.reshape(shard_count, shard_len, key_width)
    value_parts = whole_values.reshape(shard_count, shard_len, value_width)
    state = absorb_all(
        state,
        key_parts[:, :tok_rows].reshape(shard_count * tok_rows, key_width),
        value_parts[:, :tok_rows].reshape(shard_count * tok_rows, value_width),
        queries,
        head_count,
        tok_rows,
    )
    held_keys = key_parts[:, tok_rows:].reshape(shard_count * context_dev, key_width)
    held_values = value_parts[:, tok_rows:].reshape(shard_count * context_dev, value_width)
    final = absorb_all(state, held_keys, held_values, queries, head_count, context_total)
    totals = final[1]
    numerator = final[2]
    mixed = numerator[0] / totals[0][..., None] - lambda_heads[:, None, None] * (
        numerator[1] / totals[1][..., None]
    )
    normed = rms_scale(mixed) * out_gain.reshape(head_count, 1, VALUE_DIM)
    heads_out = (
        normed.transpose(1, 0, 2).reshape(tok_rows, head_count * VALUE_DIM).astype(jnp.bfloat16)
    )
    summed = lax.psum_scatter(
        jnp.dot(heads_out, out_weight, preferred_element_type=jnp.float32).astype(jnp.bfloat16),
        "tp",
        scatter_dimension=0,
        tiled=True,
    ).astype(jnp.float32)
    return (latent.astype(jnp.float32) + whole_mod[4] * summed).astype(jnp.bfloat16)


def query_slots_of(heads):
    return (tuple(range(heads)),)


def vmem(count):
    return [pl.BlockSpec(memory_space=pltpu.VMEM)] * count


SMEM = pl.BlockSpec(memory_space=pltpu.SMEM)


def cost(flops, moved):
    return pl.CostEstimate(flops=flops, bytes_accessed=moved, transcendentals=0)


def params():
    return pltpu.CompilerParams(vmem_limit_bytes=56 * 1024 * 1024)


def modulation_kernel(lam, cond_latent, cond_context, shift_w, scale_w, gate_w, gain, out):
    mod_rows = shift_w.shape[0]
    sp = lax.axis_index("sp")
    own = pl.ds(pl.multiple_of(sp * mod_rows, LANES), mod_rows)
    rows = lax.broadcasted_iota(jnp.int32, (8, mod_rows), 0)
    cond = jnp.where(rows == 0, cond_latent[:, own], cond_context[:, own])
    cond = (cond / (1.0 + jnp.exp(-cond))).astype(jnp.bfloat16)
    dot = functools.partial(jnp.dot, preferred_element_type=jnp.float32)
    out[0:2, :] = dot(cond, shift_w[...])[0:2]
    out[2:4, :] = dot(cond, scale_w[...])[0:2]
    out[4:5, :] = dot(cond, gate_w[...])[0:1]
    first = sp == 0
    out[5:6, :] = jnp.where(first, gain[...], 0.0)
    lane = lax.broadcasted_iota(jnp.int32, gain.shape, 1)
    lam_row = jnp.zeros(gain.shape, jnp.float32)
    for head in range(lam.shape[0]):
        lam_row = jnp.where(lane == head, lam[head], lam_row)
    out[6:7, :] = jnp.where(first, lam_row, 0.0)
    out[7:8, :] = jnp.zeros_like(gain)


def project_kernel(head_count, *refs):
    slots = refs[0:4]
    context, mods, cos_t, sin_t, query_w, key_w, value_w = refs[4:11]
    outs = refs[11 : 11 + head_count]
    hidden, ready = refs[11 + head_count :]
    own_rows = slots[0].shape[0]
    tok = 4 * own_rows
    ctx = context.shape[0]
    shift_l, shift_c = mods[0:1, :], mods[1:2, :]
    scale_l, scale_c = 1.0 + mods[2:3, :], 1.0 + mods[3:4, :]

    def modulate(block, scale, shift):
        v = block.astype(jnp.float32)
        r = lax.rsqrt(jnp.mean(v * v, axis=-1, keepdims=True) + norm_eps)
        return (v * r * scale + shift).astype(jnp.bfloat16)

    for index, slot in enumerate(slots):
        hidden[index * own_rows : (index + 1) * own_rows, :] = modulate(slot[...], scale_l, shift_l)
    hidden[tok:, :] = modulate(context[...], scale_c, shift_c)
    dot = functools.partial(jnp.dot, preferred_element_type=jnp.float32)

    def turned(tile):
        lane = lax.broadcasted_iota(jnp.int32, tile.shape, 1)
        swapped = jnp.where(
            lane % HEAD_DIM < HEAD_DIM // 2,
            pltpu.roll(tile, LANES - HEAD_DIM // 2, 1),
            pltpu.roll(tile, HEAD_DIM // 2, 1),
        )
        return tile * cos_t[...] + swapped * sin_t[...]

    def joined(first, second, odd):
        lane = lax.broadcasted_iota(jnp.int32, first.shape, 1)
        if odd:
            return jnp.where(lane < HEAD_DIM, pltpu.roll(first, HEAD_DIM, 1), second)
        return jnp.where(lane < HEAD_DIM, first, pltpu.roll(second, HEAD_DIM, 1))

    per_tile = LANES // HEAD_DIM
    for weight, base, count in ((query_w, 0, tok), (key_w, tok, tok + ctx)):
        first = dot(hidden[:count, :], weight[0])
        second = dot(hidden[:count, :], weight[1])
        for head in range(head_count):
            cols = slice(head // per_tile * LANES, (head // per_tile + 1) * LANES)
            whole = joined(first[:, cols], second[:, cols], head % per_tile)
            ready[head, base : base + tok, :] = turned(whole[:tok]).astype(jnp.bfloat16)
            if count > tok:
                ready[head, base + tok : base + count, :] = whole[tok:].astype(jnp.bfloat16)
    base = 2 * tok + ctx
    wide = 2 * VALUE_DIM
    for pair in range(head_count // 2):
        both = dot(hidden[...], value_w[:, pair * wide : (pair + 1) * wide]).astype(jnp.bfloat16)
        ready[2 * pair, base:, :] = both[:, :VALUE_DIM]
        ready[2 * pair + 1, base:, :] = both[:, VALUE_DIM:]
    low = lax.axis_index("sp") % head_count
    for k in range(head_count):
        outs[k][...] = ready[low ^ k]


def attention_kernel(head_count, tok, ctx, query_slots, *refs):
    whole = refs[0:head_count]
    swapped = refs[head_count : 2 * head_count]
    mods = refs[2 * head_count]
    outs = refs[2 * head_count + 1 : 2 * head_count + 1 + len(query_slots)]
    queries, keys, values, results, scores_a, scores_b, top_a, top_b, weights = refs[
        2 * head_count + 1 + len(query_slots) :
    ]
    part = tok + ctx
    for index, k in enumerate(query_slots):
        queries[index * tok : (index + 1) * tok, :] = whole[k][:tok, :]
    for k in range(head_count):
        for place_of, ref, base in ((k, whole[k], tok), (head_count + k, swapped[k], 0)):
            rows = slice(place_of * part, (place_of + 1) * part)
            keys[rows, :] = ref[base : base + part, :]
            values[rows, :LANES] = ref[base + part : base + 2 * part, :]
    ones = lax.broadcasted_iota(jnp.int32, (keys.shape[0], LANES), 1) == 0
    values[:, LANES:] = ones.astype(jnp.float32).astype(jnp.bfloat16)
    sp, tp = lax.axis_index("sp"), lax.axis_index("tp")
    head = sp % head_count
    owner = tp - tp % 2 + sp // head_count
    width = head_count * VALUE_DIM
    gain = mods[5:6, pl.ds(pl.multiple_of((owner * head_count + head) * VALUE_DIM, LANES), VALUE_DIM)]
    lam_row = mods[6:7, pl.ds(pl.multiple_of(owner * width, LANES), LANES)]
    lane_row = lax.broadcasted_iota(jnp.int32, lam_row.shape, 1)
    lam = jnp.sum(jnp.where(lane_row == head, lam_row, 0.0), axis=-1, keepdims=True)
    factor = HEAD_DIM ** (-0.5) * math.log2(math.e)
    block = scores_a.shape[0] // 2
    blocks = queries.shape[0] // block
    lane = lax.broadcasted_iota(jnp.int32, (block, LANES), 1)
    span = keys.shape[0]

    def score(index, scores, top):
        q = queries[pl.ds(pl.multiple_of(index * block, block), block), :]
        zero = jnp.zeros_like(q)
        both = jnp.concatenate(
            [jnp.where(lane < HEAD_DIM, q, zero), jnp.where(lane < HEAD_DIM, zero, q)], axis=0
        )
        result = lax.dot_general(
            both, keys[...], (((1,), (1,)), ((), ())), preferred_element_type=jnp.float32
        )
        scores[...] = result
        running = result[:, :LANES]
        for start in range(LANES, span, LANES):
            running = jnp.maximum(running, result[:, start : start + LANES])
        top[...] = jnp.broadcast_to(jnp.max(running, axis=-1, keepdims=True), top.shape)

    def absorb_block(index, scores, top):
        weights[...] = jnp.exp2((scores[...] - top[:, 0:1]) * factor).astype(jnp.bfloat16)
        sums = jnp.dot(weights[...], values[...], preferred_element_type=jnp.float32)
        share = sums[:, :LANES] / sums[:, LANES : LANES + 1]
        mixed = share[:block] - lam * share[block:]
        norm = lax.rsqrt(jnp.mean(mixed * mixed, axis=-1, keepdims=True) + norm_eps)
        rows = pl.ds(pl.multiple_of(index * block, block), block)
        results[rows, :] = (mixed * norm * gain).astype(jnp.bfloat16)

    score(0, scores_a, top_a)

    def step(pair, carry):
        index = 2 * pair
        score(jnp.minimum(index + 1, blocks - 1), scores_b, top_b)
        absorb_block(index, scores_a, top_a)
        score(jnp.minimum(index + 2, blocks - 1), scores_a, top_a)
        absorb_block(jnp.minimum(index + 1, blocks - 1), scores_b, top_b)
        return carry

    lax.fori_loop(0, pl.cdiv(blocks, 2), step, 0)
    for index in range(len(query_slots)):
        outs[index][...] = results[index * tok : (index + 1) * tok, :]


def output_kernel(*refs):
    terms = refs[0:4]
    weights = refs[4:8]
    latent, mods, out = refs[8:11]
    total = None
    for term, weight in zip(terms, weights):
        group = jnp.dot(term[...], weight[...], preferred_element_type=jnp.float32)
        group = group.astype(jnp.bfloat16).astype(jnp.float32)
        total = group if total is None else total + group
    out[...] = (latent[...].astype(jnp.float32) + mods[4:5, :] * total).astype(jnp.bfloat16)


def local_owner(
    sp_size,
    latent,
    context,
    cond_latent,
    cond_context,
    shift_weight,
    scale_weight,
    gate_weight,
    query_weight,
    key_weight,
    value_weight,
    out_weight,
    lambda_heads,
    out_gain,
):
    axes = ("sp", "tp")
    tp_size = 4
    heads = lambda_heads.shape[0]
    own_rows, width = latent.shape
    tok = tp_size * own_rows
    ctx = context.shape[0]
    f32, bf16 = jnp.float32, jnp.bfloat16
    sp = lax.axis_index("sp")
    tp = lax.axis_index("tp")
    low = sp % heads

    def hop(array, target):
        pairs = []
        for s in range(sp_size):
            for t in range(tp_size):
                s2, t2 = target(s, t)
                pairs.append((s * tp_size + t, s2 * tp_size + t2))
        return lax.ppermute(array, axes, pairs)

    def across(array, bit):
        return hop(array, lambda s, t: (s, t ^ bit))

    def to_owner(k):
        return lambda s, t: ((t % 2) * heads + ((s % heads) ^ k), t - t % 2 + s // heads)

    mod_part = pl.pallas_call(
        modulation_kernel,
        out_shape=jax.ShapeDtypeStruct((8, shift_weight.shape[1]), f32),
        in_specs=[SMEM] + vmem(6),
        out_specs=vmem(1)[0],
        compiler_params=params(),
        cost_estimate=cost(10**9, 10**6),
        name="modulation",
    )(
        lambda_heads,
        cond_latent[None, :],
        cond_context[None, :],
        shift_weight,
        scale_weight,
        gate_weight,
        out_gain[None, :],
    )

    lat_x = across(latent, 2)
    lat_c = across(latent, 1)
    step = 1
    while step < sp_size:
        mod_part = mod_part + hop(mod_part, lambda s, t, step=step: (s ^ step, t))
        step *= 2
    mods = lax.all_gather(mod_part, "tp", axis=1, tiled=True)
    lat_xc = across(lat_x, 1)
    slots = (latent, lat_x, lat_c, lat_xc)
    slot_bits = (0, 2, 1, 3)

    positions = jnp.concatenate(
        [sp * tok + (tp ^ bit) * own_rows + jnp.arange(own_rows, dtype=jnp.int32) for bit in slot_bits]
    )
    cos_half, sin_half = rope_tables(positions, GRID_W, HEAD_DIM)
    cos_t = jnp.concatenate([cos_half] * (2 * LANES // HEAD_DIM), axis=-1)
    sin_t = jnp.concatenate([-sin_half, sin_half] * (LANES // HEAD_DIM), axis=-1)

    part = tok + ctx
    message = jax.ShapeDtypeStruct((tok + 2 * part, LANES), bf16)
    messages = pl.pallas_call(
        functools.partial(project_kernel, heads),
        out_shape=[message] * heads,
        in_specs=vmem(11),
        out_specs=vmem(heads),
        scratch_shapes=[
            pltpu.VMEM((part, width), bf16),
            pltpu.VMEM((heads,) + message.shape, bf16),
        ],
        compiler_params=params(),
        cost_estimate=cost(2 * part * width * 6 * heads * HEAD_DIM, 8 * 10**6),
        name="project",
    )(*slots, context, mods, cos_t, sin_t, query_weight, key_weight, value_weight)

    arrived = [hop(messages[k], to_owner(k)) for k in range(heads)]
    swapped = [across(arrived[k][tok:], 1) for k in range(heads)]

    results = []
    for slots_of in query_slots_of(heads):
        results += pl.pallas_call(
            functools.partial(attention_kernel, heads, tok, ctx, slots_of),
            out_shape=[jax.ShapeDtypeStruct((tok, LANES), bf16)] * len(slots_of),
            in_specs=vmem(2 * heads + 1),
            out_specs=vmem(len(slots_of)),
            scratch_shapes=[
                pltpu.VMEM((len(slots_of) * tok, LANES), bf16),
                pltpu.VMEM((2 * heads * part, LANES), bf16),
                pltpu.VMEM((2 * heads * part, 2 * LANES), bf16),
                pltpu.VMEM((len(slots_of) * tok, LANES), bf16),
                pltpu.VMEM((2 * query_block, 2 * heads * part), f32),
                pltpu.VMEM((2 * query_block, 2 * heads * part), f32),
                pltpu.VMEM((2 * query_block, LANES), f32),
                pltpu.VMEM((2 * query_block, LANES), f32),
                pltpu.VMEM((2 * query_block, 2 * heads * part), bf16),
            ],
            compiler_params=params(),
            cost_estimate=cost(2 * 2 * len(slots_of) * tok * 2 * heads * part * 4 * LANES, 4 * 10**6),
            name="attention",
        )(*arrived, *swapped, mods)

    back = [hop(results[k], to_owner(k)) for k in range(heads)]
    stacked = jnp.stack(back)
    ordered = jnp.concatenate(
        [lax.dynamic_index_in_dim(stacked, low ^ m, 0, keepdims=False) for m in range(heads)], axis=1
    )
    pieces = [ordered[i * own_rows : (i + 1) * own_rows] for i in range(tp_size)]
    terms = [pieces[0]] + [across(pieces[i], slot_bits[i]) for i in range(1, tp_size)]

    late_weight, _ = lax.optimization_barrier((out_weight, mods))
    weight_x = across(late_weight, 2)
    weight_c = across(late_weight, 1)
    weight_xc = across(weight_x, 1)
    return pl.pallas_call(
        output_kernel,
        out_shape=jax.ShapeDtypeStruct(latent.shape, bf16),
        in_specs=vmem(10),
        out_specs=vmem(1)[0],
        compiler_params=params(),
        cost_estimate=cost(2 * own_rows * width * width, 8 * 10**6),
        name="output",
    )(*terms, out_weight, weight_x, weight_c, weight_xc, latent, mods)


def solution(mesh):
    placed = (
        P(("sp", "tp"), None),
        P("sp", None),
        P(),
        P(),
        P("sp", "tp"),
        P("sp", "tp"),
        P("sp", "tp"),
        P(None, None, "tp"),
        P(None, None, "tp"),
        P(None, "tp"),
        P("tp", None),
        P("tp"),
        P("tp"),
    )
    sp_size, tp_size = mesh.shape["sp"], mesh.shape["tp"]

    def local(*args):
        heads = args[11].shape[0]
        own_rows = args[0].shape[0]
        owner_plan = (
            tp_size == 4
            and sp_size == 2 * heads
            and heads % 2 == 0
            and heads & (heads - 1) == 0
            and 2 * HEAD_DIM == LANES
            and VALUE_DIM == LANES
            and own_rows % 32 == 0
            and (heads * tp_size * own_rows) % query_block == 0
            and args[1].shape[0] % 16 == 0
        )
        if owner_plan:
            return local_owner(sp_size, *args)
        return local_general(*args)

    return jax.shard_map(
        local, mesh=mesh, in_specs=placed, out_specs=P(("sp", "tp"), None), check_vma=False
    )
```

```python
import functools
import math

import jax
import jax.numpy as jnp
from jax import lax
from jax.experimental import pallas as pl
from jax.experimental.pallas import tpu as pltpu
from jax.sharding import PartitionSpec as P


HEAD_DIM = 64
GRID_W = 64
VALUE_DIM = 128
LANES = 128

norm_eps = 1e-06
rope_theta = 10000.0
block_limit = 1024
query_block = 128


def rms_scale(matrix):
    return matrix * lax.rsqrt(jnp.mean(matrix * matrix, axis=-1, keepdims=True) + norm_eps)


def modulated(activations, shift, scale):
    return (rms_scale(activations.astype(jnp.float32)) * (1.0 + scale) + shift).astype(jnp.bfloat16)


def rope_tables(positions, grid_width, head_dim):
    quarter = head_dim // 4
    inverse = rope_theta ** (-jnp.arange(quarter, dtype=jnp.float32) / quarter)
    grid_row = (positions // grid_width).astype(jnp.float32)
    grid_col = (positions % grid_width).astype(jnp.float32)
    angles = jnp.concatenate([grid_row[:, None] * inverse, grid_col[:, None] * inverse], axis=-1)
    return jnp.cos(angles), jnp.sin(angles)


def rotate(vectors, positions, grid_width):
    quarter = vectors.shape[-1] // 4
    cos_table, sin_table = rope_tables(positions, grid_width, vectors.shape[-1])
    cos_table = cos_table[:, None, :]
    sin_table = sin_table[:, None, :]
    former = vectors[..., : 2 * quarter]
    latter = vectors[..., 2 * quarter :]
    return jnp.concatenate(
        [former * cos_table - latter * sin_table, latter * cos_table + former * sin_table], axis=-1
    )


def absorb(carry_state, key_block, value_block, queries, head_count):
    maxima, totals, numerator = carry_state
    row_count = key_block.shape[0]
    scores = jnp.einsum(
        "mhqd,kmhd->mhqk",
        queries,
        key_block.reshape(row_count, 2, head_count, HEAD_DIM),
        preferred_element_type=jnp.float32,
    ) * HEAD_DIM ** (-0.5)
    new_maxima = jnp.maximum(maxima, jnp.max(scores, axis=-1))
    rescale = jnp.exp(maxima - new_maxima)
    weights = jnp.exp(scores - new_maxima[..., None])
    totals = totals * rescale + jnp.sum(weights, axis=-1)
    numerator = numerator * rescale[..., None] + jnp.einsum(
        "mhqk,khe->mhqe",
        weights.astype(jnp.bfloat16),
        value_block.reshape(row_count, head_count, VALUE_DIM),
        preferred_element_type=jnp.float32,
    )
    return (new_maxima, totals, numerator)


def absorb_all(carry_state, key_rows, value_rows, queries, head_count, shard_len):
    total_rows = key_rows.shape[0]
    shards = total_rows // shard_len
    shard_group = max(
        [
            candidate
            for candidate in range(1, shards + 1)
            if shards % candidate == 0 and candidate * shard_len <= block_limit
        ]
        + [1]
    )
    block_rows = shard_group * shard_len

    def absorb_block(block_index, inner_state):
        key_block = lax.dynamic_slice_in_dim(key_rows, block_index * block_rows, block_rows, 0)
        value_block = lax.dynamic_slice_in_dim(value_rows, block_index * block_rows, block_rows, 0)
        return absorb(inner_state, key_block, value_block, queries, head_count)

    return lax.fori_loop(0, total_rows // block_rows, absorb_block, carry_state)


def local_general(
    latent,
    context,
    cond_latent,
    cond_context,
    shift_weight,
    scale_weight,
    gate_weight,
    query_weight,
    key_weight,
    value_weight,
    out_weight,
    lambda_heads,
    out_gain,
):
    mod_rows = shift_weight.shape[0]
    conditions = jnp.stack([cond_latent, cond_context])
    conditions = jax.nn.silu(
        lax.dynamic_slice_in_dim(conditions, lax.axis_index("sp") * mod_rows, mod_rows, 1)
    )
    conditions = conditions.astype(jnp.bfloat16)
    partial_value = jnp.concatenate(
        [
            jnp.dot(conditions, shift_weight, preferred_element_type=jnp.float32),
            jnp.dot(conditions, scale_weight, preferred_element_type=jnp.float32),
            jnp.dot(conditions[:1], gate_weight, preferred_element_type=jnp.float32),
        ],
        axis=0,
    )
    summed_mod = lax.psum(partial_value, "sp")
    whole_mod = lax.all_gather(summed_mod, "tp", axis=1, tiled=True)
    hidden = modulated(latent, whole_mod[0], whole_mod[2])
    context_hidden = modulated(context, whole_mod[1], whole_mod[3])
    head_count = lambda_heads.shape[0]
    own_rows = latent.shape[0]
    tok_rows = own_rows * lax.axis_size("tp")
    row_offset = lax.axis_index("sp") * tok_rows
    piece_rows = lax.all_gather(hidden, "tp", axis=0, tiled=True)
    row_count = piece_rows.shape[0]
    positions = row_offset + jnp.arange(row_count, dtype=jnp.int32)

    def rotated(weight):
        product = jnp.concatenate(
            [
                jnp.dot(piece_rows, weight[0], preferred_element_type=jnp.float32),
                jnp.dot(piece_rows, weight[1], preferred_element_type=jnp.float32),
            ],
            axis=-1,
        )
        turned = rotate(product.reshape(row_count, 2 * head_count, HEAD_DIM), positions, GRID_W)
        return turned.reshape(row_count, 2 * head_count * HEAD_DIM).astype(jnp.bfloat16)

    values = jnp.dot(piece_rows, value_weight, preferred_element_type=jnp.float32).astype(
        jnp.bfloat16
    )
    key_width = 2 * head_count * HEAD_DIM
    queries = rotated(query_weight).reshape(tok_rows, 2, head_count, HEAD_DIM).transpose(1, 2, 0, 3)
    latent_keys = rotated(key_weight)
    context_keys = jnp.concatenate(
        [
            jnp.dot(context_hidden, key_weight[0], preferred_element_type=jnp.float32),
            jnp.dot(context_hidden, key_weight[1], preferred_element_type=jnp.float32),
        ],
        axis=-1,
    ).astype(jnp.bfloat16)
    context_values = jnp.dot(
        context_hidden, value_weight, preferred_element_type=jnp.float32
    ).astype(jnp.bfloat16)
    state = (
        jnp.full((2, head_count, tok_rows), -jnp.inf, jnp.float32),
        jnp.zeros((2, head_count, tok_rows), jnp.float32),
        jnp.zeros((2, head_count, tok_rows, VALUE_DIM), jnp.float32),
    )
    context_dev = context_keys.shape[0]
    shard_len = tok_rows + context_dev
    value_width = context_values.shape[1]
    context_total = context_dev * lax.axis_size("sp")
    whole_keys = lax.all_gather(jnp.concatenate([latent_keys, context_keys], axis=0), "sp", axis=0, tiled=True)
    whole_values = lax.all_gather(jnp.concatenate([values, context_values], axis=0), "sp", axis=0, tiled=True)
    shard_count = whole_keys.shape[0] // shard_len
    key_parts = whole_keys.reshape(shard_count, shard_len, key_width)
    value_parts = whole_values.reshape(shard_count, shard_len, value_width)
    state = absorb_all(
        state,
        key_parts[:, :tok_rows].reshape(shard_count * tok_rows, key_width),
        value_parts[:, :tok_rows].reshape(shard_count * tok_rows, value_width),
        queries,
        head_count,
        tok_rows,
    )
    held_keys = key_parts[:, tok_rows:].reshape(shard_count * context_dev, key_width)
    held_values = value_parts[:, tok_rows:].reshape(shard_count * context_dev, value_width)
    final = absorb_all(state, held_keys, held_values, queries, head_count, context_total)
    totals = final[1]
    numerator = final[2]
    mixed = numerator[0] / totals[0][..., None] - lambda_heads[:, None, None] * (
        numerator[1] / totals[1][..., None]
    )
    normed = rms_scale(mixed) * out_gain.reshape(head_count, 1, VALUE_DIM)
    heads_out = (
        normed.transpose(1, 0, 2).reshape(tok_rows, head_count * VALUE_DIM).astype(jnp.bfloat16)
    )
    summed = lax.psum_scatter(
        jnp.dot(heads_out, out_weight, preferred_element_type=jnp.float32).astype(jnp.bfloat16),
        "tp",
        scatter_dimension=0,
        tiled=True,
    ).astype(jnp.float32)
    return (latent.astype(jnp.float32) + whole_mod[4] * summed).astype(jnp.bfloat16)


def slot_head(sp, e, j):
    return (sp // 4 ^ e) * 2 + (sp % 2 ^ j)


def vmem(count):
    return [pl.BlockSpec(memory_space=pltpu.VMEM)] * count


SMEM = pl.BlockSpec(memory_space=pltpu.SMEM)
HBM = pl.BlockSpec(memory_space=pltpu.HBM)
SLOTS = ((1, 0), (1, 1), (0, 0), (0, 1))


def cost(flops, moved):
    return pl.CostEstimate(flops=flops, bytes_accessed=moved, transcendentals=0)


def params(mebibytes):
    return pltpu.CompilerParams(vmem_limit_bytes=mebibytes * 1024 * 1024)


def modulation_kernel(lam, cond_latent, cond_context, shift_w, scale_w, gate_w, gain, out):
    mod_rows = shift_w.shape[0]
    sp = lax.axis_index("sp")
    own = pl.ds(pl.multiple_of(sp * mod_rows, LANES), mod_rows)
    rows = lax.broadcasted_iota(jnp.int32, (8, mod_rows), 0)
    cond = jnp.where(rows == 0, cond_latent[:, own], cond_context[:, own])
    cond = (cond / (1.0 + jnp.exp(-cond))).astype(jnp.bfloat16)
    dot = functools.partial(jnp.dot, preferred_element_type=jnp.float32)
    out[0:2, :] = dot(cond, shift_w[...])[0:2]
    out[2:4, :] = dot(cond, scale_w[...])[0:2]
    out[4:5, :] = dot(cond, gate_w[...])[0:1]
    first = sp == 0
    out[5:6, :] = jnp.where(first, gain[...], 0.0)
    lane = lax.broadcasted_iota(jnp.int32, gain.shape, 1)
    lam_row = jnp.zeros(gain.shape, jnp.float32)
    for head in range(lam.shape[0]):
        lam_row = jnp.where(lane == head, lam[head], lam_row)
    out[6:7, :] = jnp.where(first, lam_row, 0.0)
    out[7:8, :] = jnp.zeros_like(gain)


def project_kernel(head_count, *refs):
    slots = refs[0:4]
    context, mods, cos_t, sin_t, query_w, key_w, value_w = refs[4:11]
    far_queries, far_pairs, near = refs[11:13], refs[13:15], refs[15:17]
    hidden, ready, query_v, key_v, value_v, sems = refs[17:]
    loads = [
        pltpu.make_async_copy(source, held, sems.at[index])
        for index, (source, held) in enumerate(
            ((query_w, query_v), (key_w, key_v), (value_w, value_v))
        )
    ]
    for load in loads:
        load.start()
    own_rows = slots[0].shape[0]
    tok = 4 * own_rows
    ctx = context.shape[0]
    shift_l, shift_c = mods[0:1, :], mods[1:2, :]
    scale_l, scale_c = 1.0 + mods[2:3, :], 1.0 + mods[3:4, :]

    def modulate(block, scale, shift):
        v = block.astype(jnp.float32)
        r = lax.rsqrt(jnp.mean(v * v, axis=-1, keepdims=True) + norm_eps)
        return (v * r * scale + shift).astype(jnp.bfloat16)

    for index, slot in enumerate(slots):
        hidden[index * own_rows : (index + 1) * own_rows, :] = modulate(slot[...], scale_l, shift_l)
    hidden[tok:, :] = modulate(context[...], scale_c, shift_c)
    dot = functools.partial(jnp.dot, preferred_element_type=jnp.float32)

    def turned(tile):
        lane = lax.broadcasted_iota(jnp.int32, tile.shape, 1)
        swapped = jnp.where(
            lane % HEAD_DIM < HEAD_DIM // 2,
            pltpu.roll(tile, LANES - HEAD_DIM // 2, 1),
            pltpu.roll(tile, HEAD_DIM // 2, 1),
        )
        return tile * cos_t[...] + swapped * sin_t[...]

    def joined(first, second, odd):
        lane = lax.broadcasted_iota(jnp.int32, first.shape, 1)
        if odd:
            return jnp.where(lane < HEAD_DIM, pltpu.roll(first, HEAD_DIM, 1), second)
        return jnp.where(lane < HEAD_DIM, first, pltpu.roll(second, HEAD_DIM, 1))

    per_tile = LANES // HEAD_DIM
    for load, weight, base, count in (
        (loads[0], query_v, 0, tok),
        (loads[1], key_v, tok, tok + ctx),
    ):
        load.wait()
        first = dot(hidden[:count, :], weight[0])
        second = dot(hidden[:count, :], weight[1])
        for head in range(head_count):
            cols = slice(head // per_tile * LANES, (head // per_tile + 1) * LANES)
            whole = joined(first[:, cols], second[:, cols], head % per_tile)
            ready[head, base : base + tok, :] = turned(whole[:tok]).astype(jnp.bfloat16)
            if count > tok:
                ready[head, base + tok : base + count, :] = whole[tok:].astype(jnp.bfloat16)
    base = 2 * tok + ctx
    wide = 2 * VALUE_DIM
    loads[2].wait()
    for pair in range(head_count // 2):
        both = dot(hidden[...], value_v[:, pair * wide : (pair + 1) * wide]).astype(jnp.bfloat16)
        ready[2 * pair, base:, :] = both[:, :VALUE_DIM]
        ready[2 * pair + 1, base:, :] = both[:, VALUE_DIM:]
    sp = lax.axis_index("sp")
    for j in range(2):
        near[j][...] = ready[slot_head(sp, 0, j)]
        far_queries[j][...] = ready[slot_head(sp, 1, j), :tok, :]
        far_pairs[j][...] = ready[slot_head(sp, 1, j), tok:, :]


def attention_kernel(head_count, tok, part, first, last, query_count, *refs):
    refs = list(refs)
    query_refs = [refs.pop(0) for _ in range(query_count)]
    pair_refs = [refs.pop(0) for _ in range(4)]
    if not first:
        sums_in, tops_in = refs.pop(0), refs.pop(0)
    if last:
        mods = refs.pop(0)
        outs = [refs.pop(0) for _ in range(query_count)]
    else:
        states = [(refs.pop(0), refs.pop(0)) for _ in range(2)]
    queries, keys, values, scores_a, scores_b, top_a, top_b, weights, shares = refs
    span = 4 * part
    for index, ref in enumerate(query_refs):
        queries[index * tok : (index + 1) * tok, :] = ref[:tok, :]
    for index, ref in enumerate(pair_refs):
        rows = slice(index * part, (index + 1) * part)
        offset = ref.shape[0] - 2 * part
        keys[rows, :] = ref[offset : offset + part, :]
        values[rows, :LANES] = ref[offset + part :, :]
    ones = lax.broadcasted_iota(jnp.int32, (span, LANES), 1) == 0
    values[:, LANES:] = ones.astype(jnp.float32).astype(jnp.bfloat16)
    factor = HEAD_DIM ** (-0.5) * math.log2(math.e)
    block = query_block
    blocks = query_count * tok // block
    lane = lax.broadcasted_iota(jnp.int32, (block, LANES), 1)
    if last:
        sp, tp = lax.axis_index("sp"), lax.axis_index("tp")
        head = sp // 4 * 2 + sp % 2
        owner = tp - tp % 2 + sp // 2 % 2
        width = head_count * VALUE_DIM
        start = pl.multiple_of((owner * head_count + head) * VALUE_DIM, LANES)
        gain = mods[5:6, pl.ds(start, VALUE_DIM)]
        lam_row = mods[6:7, pl.ds(pl.multiple_of(owner * width, LANES), LANES)]
        lane_row = lax.broadcasted_iota(jnp.int32, lam_row.shape, 1)
        lam = jnp.sum(jnp.where(lane_row == head, lam_row, 0.0), axis=-1, keepdims=True)

    def at(index, size):
        return pl.ds(pl.multiple_of(index * size, size), size) if not isinstance(index, int) else pl.ds(index * size, size)

    def score(index, scores, top):
        q = queries[at(index, block), :]
        zero = jnp.zeros_like(q)
        both = jnp.concatenate(
            [jnp.where(lane < HEAD_DIM, q, zero), jnp.where(lane < HEAD_DIM, zero, q)], axis=0
        )
        result = lax.dot_general(
            both, keys[...], (((1,), (1,)), ((), ())), preferred_element_type=jnp.float32
        )
        scores[...] = result
        running = result[:, :LANES]
        for start in range(LANES, span, LANES):
            running = jnp.maximum(running, result[:, start : start + LANES])
        top[...] = jnp.broadcast_to(jnp.max(running, axis=-1, keepdims=True), top.shape)

    wide_lane = lax.broadcasted_iota(jnp.int32, (2 * block, LANES), 1)

    def absorb_block(index, scores, top, state=None, origin=0):
        highest = top[...]
        if not first:
            rows = at(index, 2 * block)
            held = tops_in[rows, :]
            before = jnp.broadcast_to(held[:, :1], held.shape)
            highest = jnp.maximum(highest, before)
            shrink = jnp.exp2((before - highest) * factor)
        for start in range(0, span, LANES):
            tile = (scores[:, start : start + LANES] - highest) * factor
            weights[:, start : start + LANES] = jnp.exp2(tile).astype(jnp.bfloat16)
        both = jnp.dot(weights[...], values[...], preferred_element_type=jnp.float32)
        sums, total = both[:, :LANES], both[:, LANES : LANES + 1]
        if not first:
            sums = sums + sums_in[rows, :] * shrink
            total = total + held[:, LANES - 1 :] * shrink[:, :1]
        if not last:
            sums_out, tops_out = state
            rows = at(index - origin, 2 * block)
            sums_out[rows, :] = sums
            tops_out[rows, :] = jnp.where(wide_lane < LANES // 2, highest, total)
            return
        for which in range(2):
            rows = at(index + which * blocks, block)
            ends = slice(which * block, (which + 1) * block)
            shares[rows, :] = sums[ends] / total[ends]

    def sweep(begin, end, state=None):
        def step(pair, carry):
            index = begin + 2 * pair
            score(index + 1, scores_b, top_b)
            absorb_block(index, scores_a, top_a, state, begin)
            score(jnp.minimum(index + 2, blocks - 1), scores_a, top_a)
            absorb_block(index + 1, scores_b, top_b, state, begin)
            return carry

        lax.fori_loop(0, (end - begin) // 2, step, 0)

    score(0, scores_a, top_a)
    if last:
        sweep(0, blocks)
        for index, out in enumerate(outs):
            first_map = shares[index * tok : (index + 1) * tok, :]
            second_map = shares[(query_count + index) * tok : (query_count + index + 1) * tok, :]
            mixed = first_map - lam * second_map
            norm = lax.rsqrt(jnp.mean(mixed * mixed, axis=-1, keepdims=True) + norm_eps)
            out[...] = (mixed * norm * gain).astype(jnp.bfloat16)
    else:
        sweep(0, blocks // 2, states[0])
        sweep(blocks // 2, blocks, states[1])


def output_kernel(*refs):
    terms, weights = refs[0:4], refs[4:8]
    latent, mods, out, ordered, held, sems = refs[8:]
    loads = [
        pltpu.make_async_copy(weight, held.at[index], sems.at[index])
        for index, weight in enumerate(weights)
    ]
    for load in loads:
        load.start()
    sp = lax.axis_index("sp")
    for index, term in enumerate(terms):
        for slot, (e, j) in enumerate(SLOTS):
            place = pl.multiple_of(slot_head(sp, e, j) * VALUE_DIM, VALUE_DIM)
            ordered[index, :, pl.ds(place, VALUE_DIM)] = term[:, slot * VALUE_DIM : (slot + 1) * VALUE_DIM]
    total = None
    for index, load in enumerate(loads):
        load.wait()
        group = jnp.dot(ordered[index], held[index], preferred_element_type=jnp.float32)
        group = group.astype(jnp.bfloat16).astype(jnp.float32)
        total = group if total is None else total + group
    out[...] = (latent[...].astype(jnp.float32) + mods[4:5, :] * total).astype(jnp.bfloat16)


def local_owner(
    sp_size,
    latent,
    context,
    cond_latent,
    cond_context,
    shift_weight,
    scale_weight,
    gate_weight,
    query_weight,
    key_weight,
    value_weight,
    out_weight,
    lambda_heads,
    out_gain,
):
    axes = ("sp", "tp")
    tp_size = 4
    heads = lambda_heads.shape[0]
    own_rows, width = latent.shape
    tok = tp_size * own_rows
    ctx = context.shape[0]
    f32, bf16 = jnp.float32, jnp.bfloat16
    sp = lax.axis_index("sp")
    tp = lax.axis_index("tp")

    def hop(array, target):
        pairs = []
        for s in range(sp_size):
            for t in range(tp_size):
                s2, t2 = target(s, t)
                pairs.append((s * tp_size + t, s2 * tp_size + t2))
        return lax.ppermute(array, axes, pairs)

    def across(array, bit):
        return hop(array, lambda s, t: (s, t ^ bit))

    def to_owner(e, j):
        def target(s, t):
            return (s // 4 ^ e) * 4 + t % 2 * 2 + (s % 2 ^ j), t - t % 2 + s // 2 % 2

        return target

    from_owner = to_owner

    mod_part = pl.pallas_call(
        modulation_kernel,
        out_shape=jax.ShapeDtypeStruct((8, shift_weight.shape[1]), f32),
        in_specs=[SMEM] + vmem(6),
        out_specs=vmem(1)[0],
        compiler_params=params(60),
        cost_estimate=cost(10**9, 10**6),
        name="modulation",
    )(
        lambda_heads,
        cond_latent[None, :],
        cond_context[None, :],
        shift_weight,
        scale_weight,
        gate_weight,
        out_gain[None, :],
    )

    lat_x = across(latent, 2)
    lat_c = across(latent, 1)
    step = 1
    mod_sums = []
    while step < sp_size:
        mod_sums.append(mod_part)
        mod_part = mod_part + hop(mod_part, lambda s, t, step=step: (s ^ step, t))
        step *= 2
    mods = lax.all_gather(mod_part, "tp", axis=1, tiled=True)
    lat_xc = across(lat_x, 1)
    slots = (latent, lat_x, lat_c, lat_xc)
    slot_bits = (0, 2, 1, 3)

    shape = (tok, LANES)
    row = lax.broadcasted_iota(jnp.int32, shape, 0)
    lane = lax.broadcasted_iota(jnp.int32, shape, 1)
    slot = row // own_rows
    bits = slot // 2 + slot % 2 * 2
    positions = sp * tok + (tp ^ bits) * own_rows + row % own_rows
    quarter = HEAD_DIM // 4
    inverse = rope_theta ** (-jnp.arange(quarter, dtype=f32) / quarter)
    inverse = jnp.tile(inverse, LANES // quarter)[None, :]
    coordinate = jnp.where(lane % (2 * quarter) < quarter, positions // GRID_W, positions % GRID_W)
    angles = coordinate.astype(f32) * inverse
    cos_t = jnp.cos(angles)
    angles, _ = lax.optimization_barrier((angles, mod_sums[1]))
    sin_t = jnp.sin(angles)
    sin_t = jnp.where(lane % HEAD_DIM < HEAD_DIM // 2, -sin_t, sin_t)

    part = tok + ctx

    def block(rows):
        return jax.ShapeDtypeStruct((rows, LANES), bf16)

    messages = pl.pallas_call(
        functools.partial(project_kernel, heads),
        out_shape=[block(tok)] * 2 + [block(2 * part)] * 2 + [block(tok + 2 * part)] * 2,
        in_specs=vmem(8) + [HBM] * 3,
        out_specs=vmem(6),
        scratch_shapes=[
            pltpu.VMEM((part, width), bf16),
            pltpu.VMEM((heads, tok + 2 * part, LANES), bf16),
            pltpu.VMEM(query_weight.shape, bf16),
            pltpu.VMEM(key_weight.shape, bf16),
            pltpu.VMEM(value_weight.shape, bf16),
            pltpu.SemaphoreType.DMA((3,)),
        ],
        compiler_params=params(56),
        cost_estimate=cost(2 * part * width * 6 * heads * HEAD_DIM, 8 * 10**6),
        name="project",
    )(*slots, context, mods, cos_t, sin_t, query_weight, key_weight, value_weight)

    far_queries = [hop(messages[j], to_owner(1, j)) for j in range(2)]
    near = [hop(messages[4 + j], to_owner(0, j)) for j in range(2)]
    far = [hop(messages[2 + j], to_owner(1, j)) for j in range(2)]
    near_swapped = [across(near[j], 1) for j in range(2)]
    far_swapped = [across(far[j], 1) for j in range(2)]

    def attend(query_refs, pairs, state, last):
        count = len(query_refs)
        shapes = [jax.ShapeDtypeStruct((heads * tok, LANES), f32)] * 4
        if last:
            shapes = [block(tok)] * count
        inputs = list(query_refs) + list(pairs) + list(state)
        if last:
            inputs.append(mods)
        return pl.pallas_call(
            functools.partial(attention_kernel, heads, tok, part, not state, last, count),
            out_shape=shapes,
            in_specs=vmem(len(inputs)),
            out_specs=vmem(len(shapes)),
            scratch_shapes=[
                pltpu.VMEM((count * tok, LANES), bf16),
                pltpu.VMEM((4 * part, LANES), bf16),
                pltpu.VMEM((4 * part, 2 * LANES), bf16),
                pltpu.VMEM((2 * query_block, 4 * part), f32),
                pltpu.VMEM((2 * query_block, 4 * part), f32),
                pltpu.VMEM((2 * query_block, LANES), f32),
                pltpu.VMEM((2 * query_block, LANES), f32),
                pltpu.VMEM((2 * query_block, 4 * part), bf16),
                pltpu.VMEM((2 * count * tok if last else 8, LANES), f32),
            ],
            compiler_params=params(24),
            cost_estimate=cost(16 * count * tok * 4 * part * LANES, 10**6),
            name="attention",
        )(*inputs)

    state = attend(far_queries + near, near + near_swapped, (), False)
    late = far + far_swapped
    results = attend(far_queries, late, state[:2], True)
    back = [hop(results[j], from_owner(1, j)) for j in range(2)]
    results = attend(near, late, state[2:], True)
    back += [hop(results[j], from_owner(0, j)) for j in range(2)]
    pieces = [
        jnp.concatenate([held[i * own_rows : (i + 1) * own_rows] for held in back], axis=1)
        for i in range(tp_size)
    ]
    terms = [pieces[0]] + [across(pieces[i], slot_bits[i]) for i in range(1, tp_size)]

    late_weight, _ = lax.optimization_barrier((out_weight, mods))
    weight_x = across(late_weight, 2)
    weight_c = across(late_weight, 1)
    weight_xc = across(weight_x, 1)
    return pl.pallas_call(
        output_kernel,
        out_shape=jax.ShapeDtypeStruct(latent.shape, bf16),
        in_specs=vmem(4) + [HBM] * 4 + vmem(2),
        out_specs=vmem(1)[0],
        scratch_shapes=[
            pltpu.VMEM((4, own_rows, heads * VALUE_DIM), bf16),
            pltpu.VMEM((4,) + out_weight.shape, bf16),
            pltpu.SemaphoreType.DMA((4,)),
        ],
        compiler_params=params(24),
        cost_estimate=cost(2 * own_rows * width * width, 8 * 10**6),
        name="output",
    )(*terms, out_weight, weight_x, weight_c, weight_xc, latent, mods)


def solution(mesh):
    placed = (
        P(("sp", "tp"), None),
        P("sp", None),
        P(),
        P(),
        P("sp", "tp"),
        P("sp", "tp"),
        P("sp", "tp"),
        P(None, None, "tp"),
        P(None, None, "tp"),
        P(None, "tp"),
        P("tp", None),
        P("tp"),
        P("tp"),
    )
    sp_size, tp_size = mesh.shape["sp"], mesh.shape["tp"]

    def local(*args):
        heads = args[11].shape[0]
        own_rows = args[0].shape[0]
        owner_plan = (
            tp_size == 4
            and sp_size == 8
            and heads == 4
            and 2 * HEAD_DIM == LANES
            and VALUE_DIM == LANES
            and own_rows % 32 == 0
            and (2 * tp_size * own_rows) % query_block == 0
            and args[1].shape[0] % 16 == 0
        )
        if owner_plan:
            return local_owner(sp_size, *args)
        return local_general(*args)

    return jax.shard_map(
        local, mesh=mesh, in_specs=placed, out_specs=P(("sp", "tp"), None), check_vma=False
    )
```

```python
import functools
import math

import jax
import jax.numpy as jnp
from jax import lax
from jax.experimental import pallas as pl
from jax.experimental.pallas import tpu as pltpu
from jax.sharding import PartitionSpec as P


HEAD_DIM = 64
GRID_W = 64
VALUE_DIM = 128
LANES = 128

norm_eps = 1e-06
rope_theta = 10000.0
block_limit = 1024
query_block = 128


def rms_scale(matrix):
    return matrix * lax.rsqrt(jnp.mean(matrix * matrix, axis=-1, keepdims=True) + norm_eps)


def modulated(activations, shift, scale):
    return (rms_scale(activations.astype(jnp.float32)) * (1.0 + scale) + shift).astype(jnp.bfloat16)


def rope_tables(positions, grid_width, head_dim):
    quarter = head_dim // 4
    inverse = rope_theta ** (-jnp.arange(quarter, dtype=jnp.float32) / quarter)
    grid_row = (positions // grid_width).astype(jnp.float32)
    grid_col = (positions % grid_width).astype(jnp.float32)
    angles = jnp.concatenate([grid_row[:, None] * inverse, grid_col[:, None] * inverse], axis=-1)
    return jnp.cos(angles), jnp.sin(angles)


def rotate(vectors, positions, grid_width):
    quarter = vectors.shape[-1] // 4
    cos_table, sin_table = rope_tables(positions, grid_width, vectors.shape[-1])
    cos_table = cos_table[:, None, :]
    sin_table = sin_table[:, None, :]
    former = vectors[..., : 2 * quarter]
    latter = vectors[..., 2 * quarter :]
    return jnp.concatenate(
        [former * cos_table - latter * sin_table, latter * cos_table + former * sin_table], axis=-1
    )


def absorb(carry_state, key_block, value_block, queries, head_count):
    maxima, totals, numerator = carry_state
    row_count = key_block.shape[0]
    scores = jnp.einsum(
        "mhqd,kmhd->mhqk",
        queries,
        key_block.reshape(row_count, 2, head_count, HEAD_DIM),
        preferred_element_type=jnp.float32,
    ) * HEAD_DIM ** (-0.5)
    new_maxima = jnp.maximum(maxima, jnp.max(scores, axis=-1))
    rescale = jnp.exp(maxima - new_maxima)
    weights = jnp.exp(scores - new_maxima[..., None])
    totals = totals * rescale + jnp.sum(weights, axis=-1)
    numerator = numerator * rescale[..., None] + jnp.einsum(
        "mhqk,khe->mhqe",
        weights.astype(jnp.bfloat16),
        value_block.reshape(row_count, head_count, VALUE_DIM),
        preferred_element_type=jnp.float32,
    )
    return (new_maxima, totals, numerator)


def absorb_all(carry_state, key_rows, value_rows, queries, head_count, shard_len):
    total_rows = key_rows.shape[0]
    shards = total_rows // shard_len
    shard_group = max(
        [
            candidate
            for candidate in range(1, shards + 1)
            if shards % candidate == 0 and candidate * shard_len <= block_limit
        ]
        + [1]
    )
    block_rows = shard_group * shard_len

    def absorb_block(block_index, inner_state):
        key_block = lax.dynamic_slice_in_dim(key_rows, block_index * block_rows, block_rows, 0)
        value_block = lax.dynamic_slice_in_dim(value_rows, block_index * block_rows, block_rows, 0)
        return absorb(inner_state, key_block, value_block, queries, head_count)

    return lax.fori_loop(0, total_rows // block_rows, absorb_block, carry_state)


def local_general(
    latent,
    context,
    cond_latent,
    cond_context,
    shift_weight,
    scale_weight,
    gate_weight,
    query_weight,
    key_weight,
    value_weight,
    out_weight,
    lambda_heads,
    out_gain,
):
    mod_rows = shift_weight.shape[0]
    conditions = jnp.stack([cond_latent, cond_context])
    conditions = jax.nn.silu(
        lax.dynamic_slice_in_dim(conditions, lax.axis_index("sp") * mod_rows, mod_rows, 1)
    )
    conditions = conditions.astype(jnp.bfloat16)
    partial_value = jnp.concatenate(
        [
            jnp.dot(conditions, shift_weight, preferred_element_type=jnp.float32),
            jnp.dot(conditions, scale_weight, preferred_element_type=jnp.float32),
            jnp.dot(conditions[:1], gate_weight, preferred_element_type=jnp.float32),
        ],
        axis=0,
    )
    summed_mod = lax.psum(partial_value, "sp")
    whole_mod = lax.all_gather(summed_mod, "tp", axis=1, tiled=True)
    hidden = modulated(latent, whole_mod[0], whole_mod[2])
    context_hidden = modulated(context, whole_mod[1], whole_mod[3])
    head_count = lambda_heads.shape[0]
    own_rows = latent.shape[0]
    tok_rows = own_rows * lax.axis_size("tp")
    row_offset = lax.axis_index("sp") * tok_rows
    piece_rows = lax.all_gather(hidden, "tp", axis=0, tiled=True)
    row_count = piece_rows.shape[0]
    positions = row_offset + jnp.arange(row_count, dtype=jnp.int32)

    def rotated(weight):
        product = jnp.concatenate(
            [
                jnp.dot(piece_rows, weight[0], preferred_element_type=jnp.float32),
                jnp.dot(piece_rows, weight[1], preferred_element_type=jnp.float32),
            ],
            axis=-1,
        )
        turned = rotate(product.reshape(row_count, 2 * head_count, HEAD_DIM), positions, GRID_W)
        return turned.reshape(row_count, 2 * head_count * HEAD_DIM).astype(jnp.bfloat16)

    values = jnp.dot(piece_rows, value_weight, preferred_element_type=jnp.float32).astype(
        jnp.bfloat16
    )
    key_width = 2 * head_count * HEAD_DIM
    queries = rotated(query_weight).reshape(tok_rows, 2, head_count, HEAD_DIM).transpose(1, 2, 0, 3)
    latent_keys = rotated(key_weight)
    context_keys = jnp.concatenate(
        [
            jnp.dot(context_hidden, key_weight[0], preferred_element_type=jnp.float32),
            jnp.dot(context_hidden, key_weight[1], preferred_element_type=jnp.float32),
        ],
        axis=-1,
    ).astype(jnp.bfloat16)
    context_values = jnp.dot(
        context_hidden, value_weight, preferred_element_type=jnp.float32
    ).astype(jnp.bfloat16)
    state = (
        jnp.full((2, head_count, tok_rows), -jnp.inf, jnp.float32),
        jnp.zeros((2, head_count, tok_rows), jnp.float32),
        jnp.zeros((2, head_count, tok_rows, VALUE_DIM), jnp.float32),
    )
    context_dev = context_keys.shape[0]
    shard_len = tok_rows + context_dev
    value_width = context_values.shape[1]
    context_total = context_dev * lax.axis_size("sp")
    whole_keys = lax.all_gather(jnp.concatenate([latent_keys, context_keys], axis=0), "sp", axis=0, tiled=True)
    whole_values = lax.all_gather(jnp.concatenate([values, context_values], axis=0), "sp", axis=0, tiled=True)
    shard_count = whole_keys.shape[0] // shard_len
    key_parts = whole_keys.reshape(shard_count, shard_len, key_width)
    value_parts = whole_values.reshape(shard_count, shard_len, value_width)
    state = absorb_all(
        state,
        key_parts[:, :tok_rows].reshape(shard_count * tok_rows, key_width),
        value_parts[:, :tok_rows].reshape(shard_count * tok_rows, value_width),
        queries,
        head_count,
        tok_rows,
    )
    held_keys = key_parts[:, tok_rows:].reshape(shard_count * context_dev, key_width)
    held_values = value_parts[:, tok_rows:].reshape(shard_count * context_dev, value_width)
    final = absorb_all(state, held_keys, held_values, queries, head_count, context_total)
    totals = final[1]
    numerator = final[2]
    mixed = numerator[0] / totals[0][..., None] - lambda_heads[:, None, None] * (
        numerator[1] / totals[1][..., None]
    )
    normed = rms_scale(mixed) * out_gain.reshape(head_count, 1, VALUE_DIM)
    heads_out = (
        normed.transpose(1, 0, 2).reshape(tok_rows, head_count * VALUE_DIM).astype(jnp.bfloat16)
    )
    summed = lax.psum_scatter(
        jnp.dot(heads_out, out_weight, preferred_element_type=jnp.float32).astype(jnp.bfloat16),
        "tp",
        scatter_dimension=0,
        tiled=True,
    ).astype(jnp.float32)
    return (latent.astype(jnp.float32) + whole_mod[4] * summed).astype(jnp.bfloat16)


def slot_head(sp, e, j):
    return (sp // 4 ^ e) * 2 + (sp % 2 ^ j)


def vmem(count):
    return [pl.BlockSpec(memory_space=pltpu.VMEM)] * count


SMEM = pl.BlockSpec(memory_space=pltpu.SMEM)
HBM = pl.BlockSpec(memory_space=pltpu.HBM)
SLOTS = ((1, 0), (1, 1), (0, 0), (0, 1))


def cost(flops, moved):
    return pl.CostEstimate(flops=flops, bytes_accessed=moved, transcendentals=0)


def params(mebibytes):
    return pltpu.CompilerParams(vmem_limit_bytes=mebibytes * 1024 * 1024)


def modulation_kernel(lam, cond_latent, cond_context, shift_w, scale_w, gate_w, gain, out):
    mod_rows = shift_w.shape[0]
    sp = lax.axis_index("sp")
    own = pl.ds(pl.multiple_of(sp * mod_rows, LANES), mod_rows)
    rows = lax.broadcasted_iota(jnp.int32, (8, mod_rows), 0)
    cond = jnp.where(rows == 0, cond_latent[:, own], cond_context[:, own])
    cond = (cond / (1.0 + jnp.exp(-cond))).astype(jnp.bfloat16)
    dot = functools.partial(jnp.dot, preferred_element_type=jnp.float32)
    out[0:2, :] = dot(cond, shift_w[...])[0:2]
    out[2:4, :] = dot(cond, scale_w[...])[0:2]
    out[4:5, :] = dot(cond, gate_w[...])[0:1]
    first = sp == 0
    out[5:6, :] = jnp.where(first, gain[...], 0.0)
    lane = lax.broadcasted_iota(jnp.int32, gain.shape, 1)
    lam_row = jnp.zeros(gain.shape, jnp.float32)
    for head in range(lam.shape[0]):
        lam_row = jnp.where(lane == head, lam[head], lam_row)
    out[6:7, :] = jnp.where(first, lam_row, 0.0)
    out[7:8, :] = jnp.zeros_like(gain)


def hold_kernel(count, *refs):
    sources, outs, sems = refs[:count], refs[count : 2 * count], refs[2 * count]
    loads = [
        pltpu.make_async_copy(source, out, sems.at[index])
        for index, (source, out) in enumerate(zip(sources, outs))
    ]
    for load in loads:
        load.start()
    for load in loads:
        load.wait()


def hold(arrays, mebibytes):
    return pl.pallas_call(
        functools.partial(hold_kernel, len(arrays)),
        out_shape=[jax.ShapeDtypeStruct(a.shape, a.dtype) for a in arrays],
        in_specs=[HBM] * len(arrays),
        out_specs=vmem(len(arrays)),
        scratch_shapes=[pltpu.SemaphoreType.DMA((len(arrays),))],
        compiler_params=params(mebibytes),
        cost_estimate=cost(10**8, 8 * 10**6),
        name="hold",
    )(*arrays)


def project_kernel(head_count, *refs):
    slots = refs[0:4]
    context, mods, cos_t, sin_t, query_w, key_w, value_w = refs[4:11]
    far_queries, far_pairs, near = refs[11:13], refs[13:15], refs[15:17]
    hidden, ready = refs[17:]
    own_rows = slots[0].shape[0]
    tok = 4 * own_rows
    ctx = context.shape[0]
    shift_l, shift_c = mods[0:1, :], mods[1:2, :]
    scale_l, scale_c = 1.0 + mods[2:3, :], 1.0 + mods[3:4, :]

    def modulate(block, scale, shift):
        v = block.astype(jnp.float32)
        r = lax.rsqrt(jnp.mean(v * v, axis=-1, keepdims=True) + norm_eps)
        return (v * r * scale + shift).astype(jnp.bfloat16)

    for index, slot in enumerate(slots):
        hidden[index * own_rows : (index + 1) * own_rows, :] = modulate(slot[...], scale_l, shift_l)
    hidden[tok:, :] = modulate(context[...], scale_c, shift_c)
    dot = functools.partial(jnp.dot, preferred_element_type=jnp.float32)

    def turned(tile):
        lane = lax.broadcasted_iota(jnp.int32, tile.shape, 1)
        swapped = jnp.where(
            lane % HEAD_DIM < HEAD_DIM // 2,
            pltpu.roll(tile, LANES - HEAD_DIM // 2, 1),
            pltpu.roll(tile, HEAD_DIM // 2, 1),
        )
        return tile * cos_t[...] + swapped * sin_t[...]

    def joined(first, second, odd):
        lane = lax.broadcasted_iota(jnp.int32, first.shape, 1)
        if odd:
            return jnp.where(lane < HEAD_DIM, pltpu.roll(first, HEAD_DIM, 1), second)
        return jnp.where(lane < HEAD_DIM, first, pltpu.roll(second, HEAD_DIM, 1))

    per_tile = LANES // HEAD_DIM
    for weight, base, count in ((query_w, 0, tok), (key_w, tok, tok + ctx)):
        first = dot(hidden[:count, :], weight[0])
        second = dot(hidden[:count, :], weight[1])
        for head in range(head_count):
            cols = slice(head // per_tile * LANES, (head // per_tile + 1) * LANES)
            whole = joined(first[:, cols], second[:, cols], head % per_tile)
            ready[head, base : base + tok, :] = turned(whole[:tok]).astype(jnp.bfloat16)
            if count > tok:
                ready[head, base + tok : base + count, :] = whole[tok:].astype(jnp.bfloat16)
    base = 2 * tok + ctx
    wide = 2 * VALUE_DIM
    for pair in range(head_count // 2):
        both = dot(hidden[...], value_w[:, pair * wide : (pair + 1) * wide]).astype(jnp.bfloat16)
        ready[2 * pair, base:, :] = both[:, :VALUE_DIM]
        ready[2 * pair + 1, base:, :] = both[:, VALUE_DIM:]
    sp = lax.axis_index("sp")
    for j in range(2):
        near[j][...] = ready[slot_head(sp, 0, j)]
        far_queries[j][...] = ready[slot_head(sp, 1, j), :tok, :]
        far_pairs[j][...] = ready[slot_head(sp, 1, j), tok:, :]


def attention_kernel(head_count, tok, part, first, last, query_count, *refs):
    refs = list(refs)
    query_refs = [refs.pop(0) for _ in range(query_count)]
    pair_refs = [refs.pop(0) for _ in range(4)]
    if not first:
        sums_in, tops_in = refs.pop(0), refs.pop(0)
    if last:
        mods = refs.pop(0)
        outs = [refs.pop(0) for _ in range(query_count)]
    else:
        states = [(refs.pop(0), refs.pop(0)) for _ in range(2)]
    queries, keys, values, scores_a, scores_b, top_a, top_b, weights, shares = refs
    span = 4 * part
    for index, ref in enumerate(query_refs):
        queries[index * tok : (index + 1) * tok, :] = ref[:tok, :]
    for index, ref in enumerate(pair_refs):
        rows = slice(index * part, (index + 1) * part)
        offset = ref.shape[0] - 2 * part
        keys[rows, :] = ref[offset : offset + part, :]
        values[rows, :LANES] = ref[offset + part :, :]
    ones = lax.broadcasted_iota(jnp.int32, (span, LANES), 1) == 0
    values[:, LANES:] = ones.astype(jnp.float32).astype(jnp.bfloat16)
    factor = HEAD_DIM ** (-0.5) * math.log2(math.e)
    block = query_block
    blocks = query_count * tok // block
    lane = lax.broadcasted_iota(jnp.int32, (block, LANES), 1)
    if last:
        sp, tp = lax.axis_index("sp"), lax.axis_index("tp")
        head = sp // 4 * 2 + sp % 2
        owner = tp - tp % 2 + sp // 2 % 2
        width = head_count * VALUE_DIM
        start = pl.multiple_of((owner * head_count + head) * VALUE_DIM, LANES)
        gain = mods[5:6, pl.ds(start, VALUE_DIM)]
        lam_row = mods[6:7, pl.ds(pl.multiple_of(owner * width, LANES), LANES)]
        lane_row = lax.broadcasted_iota(jnp.int32, lam_row.shape, 1)
        lam = jnp.sum(jnp.where(lane_row == head, lam_row, 0.0), axis=-1, keepdims=True)

    def at(index, size):
        return pl.ds(pl.multiple_of(index * size, size), size) if not isinstance(index, int) else pl.ds(index * size, size)

    def score(index, scores, top):
        q = queries[at(index, block), :]
        zero = jnp.zeros_like(q)
        both = jnp.concatenate(
            [jnp.where(lane < HEAD_DIM, q, zero), jnp.where(lane < HEAD_DIM, zero, q)], axis=0
        )
        result = lax.dot_general(
            both, keys[...], (((1,), (1,)), ((), ())), preferred_element_type=jnp.float32
        )
        scores[...] = result
        running = result[:, :LANES]
        for start in range(LANES, span, LANES):
            running = jnp.maximum(running, result[:, start : start + LANES])
        top[...] = jnp.broadcast_to(jnp.max(running, axis=-1, keepdims=True), top.shape)

    wide_lane = lax.broadcasted_iota(jnp.int32, (2 * block, LANES), 1)

    def absorb_block(index, scores, top, state=None, origin=0):
        highest = top[...]
        if not first:
            rows = at(index, 2 * block)
            held = tops_in[rows, :]
            before = jnp.broadcast_to(held[:, :1], held.shape)
            highest = jnp.maximum(highest, before)
            shrink = jnp.exp2((before - highest) * factor)
        for start in range(0, span, LANES):
            tile = (scores[:, start : start + LANES] - highest) * factor
            weights[:, start : start + LANES] = jnp.exp2(tile).astype(jnp.bfloat16)
        both = jnp.dot(weights[...], values[...], preferred_element_type=jnp.float32)
        sums, total = both[:, :LANES], both[:, LANES : LANES + 1]
        if not first:
            sums = sums + sums_in[rows, :] * shrink
            total = total + held[:, LANES - 1 :] * shrink[:, :1]
        if not last:
            sums_out, tops_out = state
            rows = at(index - origin, 2 * block)
            sums_out[rows, :] = sums
            tops_out[rows, :] = jnp.where(wide_lane < LANES // 2, highest, total)
            return
        for which in range(2):
            rows = at(index + which * blocks, block)
            ends = slice(which * block, (which + 1) * block)
            shares[rows, :] = sums[ends] / total[ends]

    def sweep(begin, end, state=None):
        def step(pair, carry):
            index = begin + 2 * pair
            score(index + 1, scores_b, top_b)
            absorb_block(index, scores_a, top_a, state, begin)
            score(jnp.minimum(index + 2, blocks - 1), scores_a, top_a)
            absorb_block(index + 1, scores_b, top_b, state, begin)
            return carry

        lax.fori_loop(0, (end - begin) // 2, step, 0)

    score(0, scores_a, top_a)
    if last:
        sweep(0, blocks)
        for index, out in enumerate(outs):
            first_map = shares[index * tok : (index + 1) * tok, :]
            second_map = shares[(query_count + index) * tok : (query_count + index + 1) * tok, :]
            mixed = first_map - lam * second_map
            norm = lax.rsqrt(jnp.mean(mixed * mixed, axis=-1, keepdims=True) + norm_eps)
            out[...] = (mixed * norm * gain).astype(jnp.bfloat16)
    else:
        sweep(0, blocks // 2, states[0])
        sweep(blocks // 2, blocks, states[1])


def output_kernel(*refs):
    terms, weights = refs[0:4], refs[4:8]
    latent, mods, out, ordered = refs[8:]
    sp = lax.axis_index("sp")
    for index, term in enumerate(terms):
        for slot, (e, j) in enumerate(SLOTS):
            place = pl.multiple_of(slot_head(sp, e, j) * VALUE_DIM, VALUE_DIM)
            ordered[index, :, pl.ds(place, VALUE_DIM)] = term[:, slot * VALUE_DIM : (slot + 1) * VALUE_DIM]
    total = None
    for index, weight in enumerate(weights):
        group = jnp.dot(ordered[index], weight[...], preferred_element_type=jnp.float32)
        group = group.astype(jnp.bfloat16).astype(jnp.float32)
        total = group if total is None else total + group
    out[...] = (latent[...].astype(jnp.float32) + mods[4:5, :] * total).astype(jnp.bfloat16)


def local_owner(
    sp_size,
    latent,
    context,
    cond_latent,
    cond_context,
    shift_weight,
    scale_weight,
    gate_weight,
    query_weight,
    key_weight,
    value_weight,
    out_weight,
    lambda_heads,
    out_gain,
):
    axes = ("sp", "tp")
    tp_size = 4
    heads = lambda_heads.shape[0]
    own_rows, width = latent.shape
    tok = tp_size * own_rows
    ctx = context.shape[0]
    f32, bf16 = jnp.float32, jnp.bfloat16
    sp = lax.axis_index("sp")
    tp = lax.axis_index("tp")

    def hop(array, target):
        pairs = []
        for s in range(sp_size):
            for t in range(tp_size):
                s2, t2 = target(s, t)
                pairs.append((s * tp_size + t, s2 * tp_size + t2))
        return lax.ppermute(array, axes, pairs)

    def across(array, bit):
        return hop(array, lambda s, t: (s, t ^ bit))

    def to_owner(e, j):
        def target(s, t):
            return (s // 4 ^ e) * 4 + t % 2 * 2 + (s % 2 ^ j), t - t % 2 + s // 2 % 2

        return target

    from_owner = to_owner

    *held_weights, held_context = hold((query_weight, key_weight, value_weight, context), 47)

    mod_part = pl.pallas_call(
        modulation_kernel,
        out_shape=jax.ShapeDtypeStruct((8, shift_weight.shape[1]), f32),
        in_specs=[SMEM] + vmem(6),
        out_specs=vmem(1)[0],
        compiler_params=params(60),
        cost_estimate=cost(10**9, 10**6),
        name="modulation",
    )(
        lambda_heads,
        cond_latent[None, :],
        cond_context[None, :],
        shift_weight,
        scale_weight,
        gate_weight,
        out_gain[None, :],
    )

    lat_x = across(latent, 2)
    lat_c = across(latent, 1)
    step = 1
    mod_sums = []
    while step < sp_size:
        mod_sums.append(mod_part)
        mod_part = mod_part + hop(mod_part, lambda s, t, step=step: (s ^ step, t))
        step *= 2
    mods = lax.all_gather(mod_part, "tp", axis=1, tiled=True)
    lat_xc = across(lat_x, 1)
    slots = (latent, lat_x, lat_c, lat_xc)
    slot_bits = (0, 2, 1, 3)

    shape = (tok, LANES)
    row = lax.broadcasted_iota(jnp.int32, shape, 0)
    lane = lax.broadcasted_iota(jnp.int32, shape, 1)
    slot = row // own_rows
    bits = slot // 2 + slot % 2 * 2
    positions = sp * tok + (tp ^ bits) * own_rows + row % own_rows
    quarter = HEAD_DIM // 4
    inverse = rope_theta ** (-jnp.arange(quarter, dtype=f32) / quarter)
    inverse = jnp.tile(inverse, LANES // quarter)[None, :]
    coordinate = jnp.where(lane % (2 * quarter) < quarter, positions // GRID_W, positions % GRID_W)
    angles = coordinate.astype(f32) * inverse
    cos_t = jnp.cos(angles)
    angles, _ = lax.optimization_barrier((angles, mod_sums[1]))
    sin_t = jnp.sin(angles)
    sin_t = jnp.where(lane % HEAD_DIM < HEAD_DIM // 2, -sin_t, sin_t)

    part = tok + ctx

    def block(rows):
        return jax.ShapeDtypeStruct((rows, LANES), bf16)

    messages = pl.pallas_call(
        functools.partial(project_kernel, heads),
        out_shape=[block(tok)] * 2 + [block(2 * part)] * 2 + [block(tok + 2 * part)] * 2,
        in_specs=vmem(11),
        out_specs=vmem(6),
        scratch_shapes=[
            pltpu.VMEM((part, width), bf16),
            pltpu.VMEM((heads, tok + 2 * part, LANES), bf16),
        ],
        compiler_params=params(28),
        cost_estimate=cost(2 * part * width * 6 * heads * HEAD_DIM, 8 * 10**6),
        name="project",
    )(*slots, held_context, mods, cos_t, sin_t, *held_weights)

    far_queries = [hop(messages[j], to_owner(1, j)) for j in range(2)]
    near = [hop(messages[4 + j], to_owner(0, j)) for j in range(2)]
    far = [hop(messages[2 + j], to_owner(1, j)) for j in range(2)]
    near_swapped = [across(near[j], 1) for j in range(2)]
    far_swapped = [across(far[j], 1) for j in range(2)]

    def attend(query_refs, pairs, state, last):
        count = len(query_refs)
        shapes = [jax.ShapeDtypeStruct((heads * tok, LANES), f32)] * 4
        if last:
            shapes = [block(tok)] * count
        inputs = list(query_refs) + list(pairs) + list(state)
        if last:
            inputs.append(mods)
        return pl.pallas_call(
            functools.partial(attention_kernel, heads, tok, part, not state, last, count),
            out_shape=shapes,
            in_specs=vmem(len(inputs)),
            out_specs=vmem(len(shapes)),
            scratch_shapes=[
                pltpu.VMEM((count * tok, LANES), bf16),
                pltpu.VMEM((4 * part, LANES), bf16),
                pltpu.VMEM((4 * part, 2 * LANES), bf16),
                pltpu.VMEM((2 * query_block, 4 * part), f32),
                pltpu.VMEM((2 * query_block, 4 * part), f32),
                pltpu.VMEM((2 * query_block, LANES), f32),
                pltpu.VMEM((2 * query_block, LANES), f32),
                pltpu.VMEM((2 * query_block, 4 * part), bf16),
                pltpu.VMEM((2 * count * tok if last else 8, LANES), f32),
            ],
            compiler_params=params(24),
            cost_estimate=cost(16 * count * tok * 4 * part * LANES, 10**6),
            name="attention",
        )(*inputs)

    state = attend(far_queries + near, near + near_swapped, (), False)
    late = far + far_swapped
    results = attend(far_queries, late, state[:2], True)
    back = [hop(results[j], from_owner(1, j)) for j in range(2)]
    results = attend(near, late, state[2:], True)
    back += [hop(results[j], from_owner(0, j)) for j in range(2)]
    pieces = [
        jnp.concatenate([held[i * own_rows : (i + 1) * own_rows] for held in back], axis=1)
        for i in range(tp_size)
    ]
    terms = [pieces[0]] + [across(pieces[i], slot_bits[i]) for i in range(1, tp_size)]

    late_weight, _ = lax.optimization_barrier((out_weight, mods))
    weight_x = across(late_weight, 2)
    weight_c = across(late_weight, 1)
    weight_xc = across(weight_x, 1)
    return pl.pallas_call(
        output_kernel,
        out_shape=jax.ShapeDtypeStruct(latent.shape, bf16),
        in_specs=vmem(10),
        out_specs=vmem(1)[0],
        scratch_shapes=[
            pltpu.VMEM((4, own_rows, heads * VALUE_DIM), bf16),
        ],
        compiler_params=params(24),
        cost_estimate=cost(2 * own_rows * width * width, 8 * 10**6),
        name="output",
    )(*terms, out_weight, weight_x, weight_c, weight_xc, latent, mods)


def solution(mesh):
    placed = (
        P(("sp", "tp"), None),
        P("sp", None),
        P(),
        P(),
        P("sp", "tp"),
        P("sp", "tp"),
        P("sp", "tp"),
        P(None, None, "tp"),
        P(None, None, "tp"),
        P(None, "tp"),
        P("tp", None),
        P("tp"),
        P("tp"),
    )
    sp_size, tp_size = mesh.shape["sp"], mesh.shape["tp"]

    def local(*args):
        heads = args[11].shape[0]
        own_rows = args[0].shape[0]
        owner_plan = (
            tp_size == 4
            and sp_size == 8
            and heads == 4
            and 2 * HEAD_DIM == LANES
            and VALUE_DIM == LANES
            and own_rows % 32 == 0
            and (2 * tp_size * own_rows) % query_block == 0
            and args[1].shape[0] % 16 == 0
        )
        if owner_plan:
            return local_owner(sp_size, *args)
        return local_general(*args)

    return jax.shard_map(
        local, mesh=mesh, in_specs=placed, out_specs=P(("sp", "tp"), None), check_vma=False
    )
```

```python
import functools
import math

import jax
import jax.numpy as jnp
from jax import lax
from jax.experimental import pallas as pl
from jax.experimental.pallas import tpu as pltpu
from jax.sharding import PartitionSpec as P


HEAD_DIM = 64
GRID_W = 64
VALUE_DIM = 128
LANES = 128

norm_eps = 1e-06
rope_theta = 10000.0
block_limit = 1024
query_block = 192


def rms_scale(matrix):
    return matrix * lax.rsqrt(jnp.mean(matrix * matrix, axis=-1, keepdims=True) + norm_eps)


def modulated(activations, shift, scale):
    return (rms_scale(activations.astype(jnp.float32)) * (1.0 + scale) + shift).astype(jnp.bfloat16)


def rope_tables(positions, grid_width, head_dim):
    quarter = head_dim // 4
    inverse = rope_theta ** (-jnp.arange(quarter, dtype=jnp.float32) / quarter)
    grid_row = (positions // grid_width).astype(jnp.float32)
    grid_col = (positions % grid_width).astype(jnp.float32)
    angles = jnp.concatenate([grid_row[:, None] * inverse, grid_col[:, None] * inverse], axis=-1)
    return jnp.cos(angles), jnp.sin(angles)


def rotate(vectors, positions, grid_width):
    quarter = vectors.shape[-1] // 4
    cos_table, sin_table = rope_tables(positions, grid_width, vectors.shape[-1])
    cos_table = cos_table[:, None, :]
    sin_table = sin_table[:, None, :]
    former = vectors[..., : 2 * quarter]
    latter = vectors[..., 2 * quarter :]
    return jnp.concatenate(
        [former * cos_table - latter * sin_table, latter * cos_table + former * sin_table], axis=-1
    )


def absorb(carry_state, key_block, value_block, queries, head_count):
    maxima, totals, numerator = carry_state
    row_count = key_block.shape[0]
    scores = jnp.einsum(
        "mhqd,kmhd->mhqk",
        queries,
        key_block.reshape(row_count, 2, head_count, HEAD_DIM),
        preferred_element_type=jnp.float32,
    ) * HEAD_DIM ** (-0.5)
    new_maxima = jnp.maximum(maxima, jnp.max(scores, axis=-1))
    rescale = jnp.exp(maxima - new_maxima)
    weights = jnp.exp(scores - new_maxima[..., None])
    totals = totals * rescale + jnp.sum(weights, axis=-1)
    numerator = numerator * rescale[..., None] + jnp.einsum(
        "mhqk,khe->mhqe",
        weights.astype(jnp.bfloat16),
        value_block.reshape(row_count, head_count, VALUE_DIM),
        preferred_element_type=jnp.float32,
    )
    return (new_maxima, totals, numerator)


def absorb_all(carry_state, key_rows, value_rows, queries, head_count, shard_len):
    total_rows = key_rows.shape[0]
    shards = total_rows // shard_len
    shard_group = max(
        [
            candidate
            for candidate in range(1, shards + 1)
            if shards % candidate == 0 and candidate * shard_len <= block_limit
        ]
        + [1]
    )
    block_rows = shard_group * shard_len

    def absorb_block(block_index, inner_state):
        key_block = lax.dynamic_slice_in_dim(key_rows, block_index * block_rows, block_rows, 0)
        value_block = lax.dynamic_slice_in_dim(value_rows, block_index * block_rows, block_rows, 0)
        return absorb(inner_state, key_block, value_block, queries, head_count)

    return lax.fori_loop(0, total_rows // block_rows, absorb_block, carry_state)


def local_general(
    latent,
    context,
    cond_latent,
    cond_context,
    shift_weight,
    scale_weight,
    gate_weight,
    query_weight,
    key_weight,
    value_weight,
    out_weight,
    lambda_heads,
    out_gain,
):
    mod_rows = shift_weight.shape[0]
    conditions = jnp.stack([cond_latent, cond_context])
    conditions = jax.nn.silu(
        lax.dynamic_slice_in_dim(conditions, lax.axis_index("sp") * mod_rows, mod_rows, 1)
    )
    conditions = conditions.astype(jnp.bfloat16)
    partial_value = jnp.concatenate(
        [
            jnp.dot(conditions, shift_weight, preferred_element_type=jnp.float32),
            jnp.dot(conditions, scale_weight, preferred_element_type=jnp.float32),
            jnp.dot(conditions[:1], gate_weight, preferred_element_type=jnp.float32),
        ],
        axis=0,
    )
    summed_mod = lax.psum(partial_value, "sp")
    whole_mod = lax.all_gather(summed_mod, "tp", axis=1, tiled=True)
    hidden = modulated(latent, whole_mod[0], whole_mod[2])
    context_hidden = modulated(context, whole_mod[1], whole_mod[3])
    head_count = lambda_heads.shape[0]
    own_rows = latent.shape[0]
    tok_rows = own_rows * lax.axis_size("tp")
    row_offset = lax.axis_index("sp") * tok_rows
    piece_rows = lax.all_gather(hidden, "tp", axis=0, tiled=True)
    row_count = piece_rows.shape[0]
    positions = row_offset + jnp.arange(row_count, dtype=jnp.int32)

    def rotated(weight):
        product = jnp.concatenate(
            [
                jnp.dot(piece_rows, weight[0], preferred_element_type=jnp.float32),
                jnp.dot(piece_rows, weight[1], preferred_element_type=jnp.float32),
            ],
            axis=-1,
        )
        turned = rotate(product.reshape(row_count, 2 * head_count, HEAD_DIM), positions, GRID_W)
        return turned.reshape(row_count, 2 * head_count * HEAD_DIM).astype(jnp.bfloat16)

    values = jnp.dot(piece_rows, value_weight, preferred_element_type=jnp.float32).astype(
        jnp.bfloat16
    )
    key_width = 2 * head_count * HEAD_DIM
    queries = rotated(query_weight).reshape(tok_rows, 2, head_count, HEAD_DIM).transpose(1, 2, 0, 3)
    latent_keys = rotated(key_weight)
    context_keys = jnp.concatenate(
        [
            jnp.dot(context_hidden, key_weight[0], preferred_element_type=jnp.float32),
            jnp.dot(context_hidden, key_weight[1], preferred_element_type=jnp.float32),
        ],
        axis=-1,
    ).astype(jnp.bfloat16)
    context_values = jnp.dot(
        context_hidden, value_weight, preferred_element_type=jnp.float32
    ).astype(jnp.bfloat16)
    state = (
        jnp.full((2, head_count, tok_rows), -jnp.inf, jnp.float32),
        jnp.zeros((2, head_count, tok_rows), jnp.float32),
        jnp.zeros((2, head_count, tok_rows, VALUE_DIM), jnp.float32),
    )
    context_dev = context_keys.shape[0]
    shard_len = tok_rows + context_dev
    value_width = context_values.shape[1]
    context_total = context_dev * lax.axis_size("sp")
    whole_keys = lax.all_gather(jnp.concatenate([latent_keys, context_keys], axis=0), "sp", axis=0, tiled=True)
    whole_values = lax.all_gather(jnp.concatenate([values, context_values], axis=0), "sp", axis=0, tiled=True)
    shard_count = whole_keys.shape[0] // shard_len
    key_parts = whole_keys.reshape(shard_count, shard_len, key_width)
    value_parts = whole_values.reshape(shard_count, shard_len, value_width)
    state = absorb_all(
        state,
        key_parts[:, :tok_rows].reshape(shard_count * tok_rows, key_width),
        value_parts[:, :tok_rows].reshape(shard_count * tok_rows, value_width),
        queries,
        head_count,
        tok_rows,
    )
    held_keys = key_parts[:, tok_rows:].reshape(shard_count * context_dev, key_width)
    held_values = value_parts[:, tok_rows:].reshape(shard_count * context_dev, value_width)
    final = absorb_all(state, held_keys, held_values, queries, head_count, context_total)
    totals = final[1]
    numerator = final[2]
    mixed = numerator[0] / totals[0][..., None] - lambda_heads[:, None, None] * (
        numerator[1] / totals[1][..., None]
    )
    normed = rms_scale(mixed) * out_gain.reshape(head_count, 1, VALUE_DIM)
    heads_out = (
        normed.transpose(1, 0, 2).reshape(tok_rows, head_count * VALUE_DIM).astype(jnp.bfloat16)
    )
    summed = lax.psum_scatter(
        jnp.dot(heads_out, out_weight, preferred_element_type=jnp.float32).astype(jnp.bfloat16),
        "tp",
        scatter_dimension=0,
        tiled=True,
    ).astype(jnp.float32)
    return (latent.astype(jnp.float32) + whole_mod[4] * summed).astype(jnp.bfloat16)


def slot_head(sp, e, j):
    return (sp // 4 ^ e) * 2 + (sp % 2 ^ j)


def vmem(count):
    return [pl.BlockSpec(memory_space=pltpu.VMEM)] * count


SMEM = pl.BlockSpec(memory_space=pltpu.SMEM)
HBM = pl.BlockSpec(memory_space=pltpu.HBM)
SLOTS = ((1, 0), (1, 1), (0, 0), (0, 1))


def cost(flops, moved):
    return pl.CostEstimate(flops=flops, bytes_accessed=moved, transcendentals=0)


def params(mebibytes):
    return pltpu.CompilerParams(vmem_limit_bytes=mebibytes * 1024 * 1024)


def modulation_kernel(lam, cond_latent, cond_context, shift_w, scale_w, gate_w, gain, out):
    mod_rows = shift_w.shape[0]
    sp = lax.axis_index("sp")
    own = pl.ds(pl.multiple_of(sp * mod_rows, LANES), mod_rows)
    rows = lax.broadcasted_iota(jnp.int32, (8, mod_rows), 0)
    cond = jnp.where(rows == 0, cond_latent[:, own], cond_context[:, own])
    cond = (cond / (1.0 + jnp.exp(-cond))).astype(jnp.bfloat16)
    dot = functools.partial(jnp.dot, preferred_element_type=jnp.float32)
    out[0:2, :] = dot(cond, shift_w[...])[0:2]
    out[2:4, :] = dot(cond, scale_w[...])[0:2]
    out[4:5, :] = dot(cond, gate_w[...])[0:1]
    first = sp == 0
    out[5:6, :] = jnp.where(first, gain[...], 0.0)
    lane = lax.broadcasted_iota(jnp.int32, gain.shape, 1)
    lam_row = jnp.zeros(gain.shape, jnp.float32)
    for head in range(lam.shape[0]):
        lam_row = jnp.where(lane == head, lam[head], lam_row)
    out[6:7, :] = jnp.where(first, lam_row, 0.0)
    out[7:8, :] = jnp.zeros_like(gain)


def hold_kernel(count, *refs):
    sources, outs, sems = refs[:count], refs[count : 2 * count], refs[2 * count]
    loads = [
        pltpu.make_async_copy(source, out, sems.at[index])
        for index, (source, out) in enumerate(zip(sources, outs))
    ]
    for load in loads:
        load.start()
    for load in loads:
        load.wait()


def hold(arrays, mebibytes):
    return pl.pallas_call(
        functools.partial(hold_kernel, len(arrays)),
        out_shape=[jax.ShapeDtypeStruct(a.shape, a.dtype) for a in arrays],
        in_specs=[HBM] * len(arrays),
        out_specs=vmem(len(arrays)),
        scratch_shapes=[pltpu.SemaphoreType.DMA((len(arrays),))],
        compiler_params=params(mebibytes),
        cost_estimate=cost(10**8, 8 * 10**6),
        name="hold",
    )(*arrays)


def project_kernel(head_count, *refs):
    slots = refs[0:4]
    context, mods, cos_t, sin_t, query_w, key_w, value_w = refs[4:11]
    far_queries, far_pairs, near = refs[11:13], refs[13:15], refs[15:17]
    hidden, ready = refs[17:]
    own_rows = slots[0].shape[0]
    tok = 4 * own_rows
    ctx = context.shape[0]
    shift_l, shift_c = mods[0:1, :], mods[1:2, :]
    scale_l, scale_c = 1.0 + mods[2:3, :], 1.0 + mods[3:4, :]

    def modulate(block, scale, shift):
        v = block.astype(jnp.float32)
        r = lax.rsqrt(jnp.mean(v * v, axis=-1, keepdims=True) + norm_eps)
        return (v * r * scale + shift).astype(jnp.bfloat16)

    for index, slot in enumerate(slots):
        hidden[index * own_rows : (index + 1) * own_rows, :] = modulate(slot[...], scale_l, shift_l)
    hidden[tok:, :] = modulate(context[...], scale_c, shift_c)
    dot = functools.partial(jnp.dot, preferred_element_type=jnp.float32)

    def turned(tile):
        lane = lax.broadcasted_iota(jnp.int32, tile.shape, 1)
        swapped = jnp.where(
            lane % HEAD_DIM < HEAD_DIM // 2,
            pltpu.roll(tile, LANES - HEAD_DIM // 2, 1),
            pltpu.roll(tile, HEAD_DIM // 2, 1),
        )
        return tile * cos_t[...] + swapped * sin_t[...]

    def joined(first, second, odd):
        lane = lax.broadcasted_iota(jnp.int32, first.shape, 1)
        if odd:
            return jnp.where(lane < HEAD_DIM, pltpu.roll(first, HEAD_DIM, 1), second)
        return jnp.where(lane < HEAD_DIM, first, pltpu.roll(second, HEAD_DIM, 1))

    per_tile = LANES // HEAD_DIM
    for weight, base, count in ((query_w, 0, tok), (key_w, tok, tok + ctx)):
        first = dot(hidden[:count, :], weight[0])
        second = dot(hidden[:count, :], weight[1])
        for head in range(head_count):
            cols = slice(head // per_tile * LANES, (head // per_tile + 1) * LANES)
            whole = joined(first[:, cols], second[:, cols], head % per_tile)
            ready[head, base : base + tok, :] = turned(whole[:tok]).astype(jnp.bfloat16)
            if count > tok:
                ready[head, base + tok : base + count, :] = whole[tok:].astype(jnp.bfloat16)
    base = 2 * tok + ctx
    wide = 2 * VALUE_DIM
    for pair in range(head_count // 2):
        both = dot(hidden[...], value_w[:, pair * wide : (pair + 1) * wide]).astype(jnp.bfloat16)
        ready[2 * pair, base:, :] = both[:, :VALUE_DIM]
        ready[2 * pair + 1, base:, :] = both[:, VALUE_DIM:]
    sp = lax.axis_index("sp")
    for j in range(2):
        near[j][...] = ready[slot_head(sp, 0, j)]
        far_queries[j][...] = ready[slot_head(sp, 1, j), :tok, :]
        far_pairs[j][...] = ready[slot_head(sp, 1, j), tok:, :]


def attention_kernel(head_count, tok, part, first, last, query_count, *refs):
    refs = list(refs)
    query_refs = [refs.pop(0) for _ in range(query_count)]
    pair_refs = [refs.pop(0) for _ in range(4)]
    if not first:
        sums_in, tops_in = refs.pop(0), refs.pop(0)
    if last:
        mods = refs.pop(0)
        outs = [refs.pop(0) for _ in range(query_count)]
    else:
        states = [(refs.pop(0), refs.pop(0)) for _ in range(2)]
    queries, keys, values, scores_a, scores_b, top_a, top_b, weights, shares = refs
    span = 4 * part
    for index, ref in enumerate(query_refs):
        queries[index * tok : (index + 1) * tok, :] = ref[:tok, :]
    for index, ref in enumerate(pair_refs):
        rows = slice(index * part, (index + 1) * part)
        offset = ref.shape[0] - 2 * part
        keys[rows, :] = ref[offset : offset + part, :]
        values[rows, :LANES] = ref[offset + part :, :]
    ones = lax.broadcasted_iota(jnp.int32, (span, LANES), 1) == 0
    values[:, LANES:] = ones.astype(jnp.float32).astype(jnp.bfloat16)
    factor = HEAD_DIM ** (-0.5) * math.log2(math.e)
    block = query_block
    blocks = query_count * tok // block
    lane = lax.broadcasted_iota(jnp.int32, (block, LANES), 1)
    if last:
        sp, tp = lax.axis_index("sp"), lax.axis_index("tp")
        head = sp // 4 * 2 + sp % 2
        owner = tp - tp % 2 + sp // 2 % 2
        width = head_count * VALUE_DIM
        start = pl.multiple_of((owner * head_count + head) * VALUE_DIM, LANES)
        gain = mods[5:6, pl.ds(start, VALUE_DIM)]
        lam_row = mods[6:7, pl.ds(pl.multiple_of(owner * width, LANES), LANES)]
        lane_row = lax.broadcasted_iota(jnp.int32, lam_row.shape, 1)
        lam = jnp.sum(jnp.where(lane_row == head, lam_row, 0.0), axis=-1, keepdims=True)

    def at(index, size):
        return pl.ds(pl.multiple_of(index * size, size), size) if not isinstance(index, int) else pl.ds(index * size, size)

    def score(index, scores, top):
        q = queries[at(index, block), :]
        zero = jnp.zeros_like(q)
        both = jnp.concatenate(
            [jnp.where(lane < HEAD_DIM, q, zero), jnp.where(lane < HEAD_DIM, zero, q)], axis=0
        )
        result = lax.dot_general(
            both, keys[...], (((1,), (1,)), ((), ())), preferred_element_type=jnp.float32
        )
        scores[...] = result
        running = result[:, :LANES]
        for start in range(LANES, span, LANES):
            running = jnp.maximum(running, result[:, start : start + LANES])
        top[...] = jnp.broadcast_to(jnp.max(running, axis=-1, keepdims=True), top.shape)

    wide_lane = lax.broadcasted_iota(jnp.int32, (2 * block, LANES), 1)

    def absorb_block(index, scores, top, state=None, origin=0):
        highest = top[...]
        if not first:
            rows = at(index, 2 * block)
            held = tops_in[rows, :]
            before = jnp.broadcast_to(held[:, :1], held.shape)
            highest = jnp.maximum(highest, before)
            shrink = jnp.exp2((before - highest) * factor)
        for start in range(0, span, LANES):
            tile = (scores[:, start : start + LANES] - highest) * factor
            weights[:, start : start + LANES] = jnp.exp2(tile).astype(jnp.bfloat16)
        both = jnp.dot(weights[...], values[...], preferred_element_type=jnp.float32)
        sums, total = both[:, :LANES], both[:, LANES : LANES + 1]
        if not first:
            sums = sums + sums_in[rows, :] * shrink
            total = total + held[:, LANES - 1 :] * shrink[:, :1]
        if not last:
            sums_out, tops_out = state
            rows = at(index - origin, 2 * block)
            sums_out[rows, :] = sums
            tops_out[rows, :] = jnp.where(wide_lane < LANES // 2, highest, total)
            return
        for which in range(2):
            rows = at(index + which * blocks, block)
            ends = slice(which * block, (which + 1) * block)
            shares[rows, :] = sums[ends] / total[ends]

    def sweep(begin, end, state=None):
        def step(pair, carry):
            index = begin + 2 * pair
            score(index + 1, scores_b, top_b)
            absorb_block(index, scores_a, top_a, state, begin)
            score(jnp.minimum(index + 2, blocks - 1), scores_a, top_a)
            absorb_block(index + 1, scores_b, top_b, state, begin)
            return carry

        lax.fori_loop(0, (end - begin) // 2, step, 0)

    score(0, scores_a, top_a)
    if last:
        sweep(0, blocks)
        for index, out in enumerate(outs):
            first_map = shares[index * tok : (index + 1) * tok, :]
            second_map = shares[(query_count + index) * tok : (query_count + index + 1) * tok, :]
            mixed = first_map - lam * second_map
            norm = lax.rsqrt(jnp.mean(mixed * mixed, axis=-1, keepdims=True) + norm_eps)
            out[...] = (mixed * norm * gain).astype(jnp.bfloat16)
    else:
        sweep(0, blocks // 2, states[0])
        sweep(blocks // 2, blocks, states[1])


def output_kernel(*refs):
    terms, weights = (refs[0:4], refs[4:8]), refs[8:12]
    latent, mods, out, ordered = refs[12:]
    sp = lax.axis_index("sp")
    for slot, (e, j) in enumerate(SLOTS):
        place = pl.ds(pl.multiple_of(slot_head(sp, e, j) * VALUE_DIM, VALUE_DIM), VALUE_DIM)
        for index in range(4):
            lanes = slice(slot % 2 * VALUE_DIM, (slot % 2 + 1) * VALUE_DIM)
            ordered[index, :, place] = terms[slot // 2][index][:, lanes]
    total = None
    for index, weight in enumerate(weights):
        group = jnp.dot(ordered[index], weight[...], preferred_element_type=jnp.float32)
        group = group.astype(jnp.bfloat16).astype(jnp.float32)
        total = group if total is None else total + group
    out[...] = (latent[...].astype(jnp.float32) + mods[4:5, :] * total).astype(jnp.bfloat16)


def local_owner(
    sp_size,
    latent,
    context,
    cond_latent,
    cond_context,
    shift_weight,
    scale_weight,
    gate_weight,
    query_weight,
    key_weight,
    value_weight,
    out_weight,
    lambda_heads,
    out_gain,
):
    axes = ("sp", "tp")
    tp_size = 4
    heads = lambda_heads.shape[0]
    own_rows, width = latent.shape
    tok = tp_size * own_rows
    ctx = context.shape[0]
    f32, bf16 = jnp.float32, jnp.bfloat16
    sp = lax.axis_index("sp")
    tp = lax.axis_index("tp")

    def hop(array, target):
        pairs = []
        for s in range(sp_size):
            for t in range(tp_size):
                s2, t2 = target(s, t)
                pairs.append((s * tp_size + t, s2 * tp_size + t2))
        return lax.ppermute(array, axes, pairs)

    def across(array, bit):
        return hop(array, lambda s, t: (s, t ^ bit))

    def to_owner(e, j):
        def target(s, t):
            return (s // 4 ^ e) * 4 + t % 2 * 2 + (s % 2 ^ j), t - t % 2 + s // 2 % 2

        return target

    from_owner = to_owner

    *held_weights, held_context = hold((query_weight, key_weight, value_weight, context), 47)

    mod_part = pl.pallas_call(
        modulation_kernel,
        out_shape=jax.ShapeDtypeStruct((8, shift_weight.shape[1]), f32),
        in_specs=[SMEM] + vmem(6),
        out_specs=vmem(1)[0],
        compiler_params=params(60),
        cost_estimate=cost(10**9, 10**6),
        name="modulation",
    )(
        lambda_heads,
        cond_latent[None, :],
        cond_context[None, :],
        shift_weight,
        scale_weight,
        gate_weight,
        out_gain[None, :],
    )

    lat_x = across(latent, 2)
    lat_c = across(latent, 1)
    step = 1
    mod_sums = []
    while step < sp_size:
        mod_sums.append(mod_part)
        mod_part = mod_part + hop(mod_part, lambda s, t, step=step: (s ^ step, t))
        step *= 2
    mods = lax.all_gather(mod_part, "tp", axis=1, tiled=True)
    lat_xc = across(lat_x, 1)
    slots = (latent, lat_x, lat_c, lat_xc)
    slot_bits = (0, 2, 1, 3)

    shape = (tok, LANES)
    row = lax.broadcasted_iota(jnp.int32, shape, 0)
    lane = lax.broadcasted_iota(jnp.int32, shape, 1)
    slot = row // own_rows
    bits = slot // 2 + slot % 2 * 2
    positions = sp * tok + (tp ^ bits) * own_rows + row % own_rows
    quarter = HEAD_DIM // 4
    inverse = rope_theta ** (-jnp.arange(quarter, dtype=f32) / quarter)
    inverse = jnp.tile(inverse, LANES // quarter)[None, :]
    coordinate = jnp.where(lane % (2 * quarter) < quarter, positions // GRID_W, positions % GRID_W)
    angles = coordinate.astype(f32) * inverse
    cos_t = jnp.cos(angles)
    angles, _ = lax.optimization_barrier((angles, mod_sums[1]))
    sin_t = jnp.sin(angles)
    sin_t = jnp.where(lane % HEAD_DIM < HEAD_DIM // 2, -sin_t, sin_t)

    part = tok + ctx

    def block(rows):
        return jax.ShapeDtypeStruct((rows, LANES), bf16)

    messages = pl.pallas_call(
        functools.partial(project_kernel, heads),
        out_shape=[block(tok)] * 2 + [block(2 * part)] * 2 + [block(tok + 2 * part)] * 2,
        in_specs=vmem(11),
        out_specs=vmem(6),
        scratch_shapes=[
            pltpu.VMEM((part, width), bf16),
            pltpu.VMEM((heads, tok + 2 * part, LANES), bf16),
        ],
        compiler_params=params(28),
        cost_estimate=cost(2 * part * width * 6 * heads * HEAD_DIM, 8 * 10**6),
        name="project",
    )(*slots, held_context, mods, cos_t, sin_t, *held_weights)

    far_queries = [hop(messages[j], to_owner(1, j)) for j in range(2)]
    near = [hop(messages[4 + j], to_owner(0, j)) for j in range(2)]
    far = [hop(messages[2 + j], to_owner(1, j)) for j in range(2)]
    near_swapped = [across(near[j], 1) for j in range(2)]
    far_swapped = [across(far[j], 1) for j in range(2)]

    def attend(query_refs, pairs, state, last):
        count = len(query_refs)
        shapes = [jax.ShapeDtypeStruct((heads * tok, LANES), f32)] * 4
        if last:
            shapes = [block(tok)] * count
        inputs = list(query_refs) + list(pairs) + list(state)
        if last:
            inputs.append(mods)
        return pl.pallas_call(
            functools.partial(attention_kernel, heads, tok, part, not state, last, count),
            out_shape=shapes,
            in_specs=vmem(len(inputs)),
            out_specs=vmem(len(shapes)),
            scratch_shapes=[
                pltpu.VMEM((count * tok, LANES), bf16),
                pltpu.VMEM((4 * part, LANES), bf16),
                pltpu.VMEM((4 * part, 2 * LANES), bf16),
                pltpu.VMEM((2 * query_block, 4 * part), f32),
                pltpu.VMEM((2 * query_block, 4 * part), f32),
                pltpu.VMEM((2 * query_block, LANES), f32),
                pltpu.VMEM((2 * query_block, LANES), f32),
                pltpu.VMEM((2 * query_block, 4 * part), bf16),
                pltpu.VMEM((2 * count * tok if last else 8, LANES), f32),
            ],
            compiler_params=params(24),
            cost_estimate=cost(16 * count * tok * 4 * part * LANES, 10**6),
            name="attention",
        )(*inputs)

    state = attend(far_queries + near, near + near_swapped, (), False)
    late = far + far_swapped
    results = attend(far_queries, late, state[:2], True)
    back = [hop(results[j], from_owner(1, j)) for j in range(2)]
    results = attend(near, late, state[2:], True)
    back += [hop(results[j], from_owner(0, j)) for j in range(2)]
    terms = []
    for held in (back[:2], back[2:]):
        pieces = [
            jnp.concatenate([part_of[i * own_rows : (i + 1) * own_rows] for part_of in held], axis=1)
            for i in range(tp_size)
        ]
        terms.append([pieces[0]] + [across(pieces[i], slot_bits[i]) for i in range(1, tp_size)])

    late_weight, _ = lax.optimization_barrier((out_weight, mods))
    weight_x = across(late_weight, 2)
    weight_c = across(late_weight, 1)
    weight_xc = across(weight_x, 1)
    return pl.pallas_call(
        output_kernel,
        out_shape=jax.ShapeDtypeStruct(latent.shape, bf16),
        in_specs=vmem(14),
        out_specs=vmem(1)[0],
        scratch_shapes=[
            pltpu.VMEM((4, own_rows, heads * VALUE_DIM), bf16),
        ],
        compiler_params=params(24),
        cost_estimate=cost(2 * own_rows * width * width, 8 * 10**6),
        name="output",
    )(*terms[0], *terms[1], out_weight, weight_x, weight_c, weight_xc, latent, mods)


def solution(mesh):
    placed = (
        P(("sp", "tp"), None),
        P("sp", None),
        P(),
        P(),
        P("sp", "tp"),
        P("sp", "tp"),
        P("sp", "tp"),
        P(None, None, "tp"),
        P(None, None, "tp"),
        P(None, "tp"),
        P("tp", None),
        P("tp"),
        P("tp"),
    )
    sp_size, tp_size = mesh.shape["sp"], mesh.shape["tp"]

    def local(*args):
        heads = args[11].shape[0]
        own_rows = args[0].shape[0]
        owner_plan = (
            tp_size == 4
            and sp_size == 8
            and heads == 4
            and 2 * HEAD_DIM == LANES
            and VALUE_DIM == LANES
            and own_rows % 32 == 0
            and (2 * tp_size * own_rows) % query_block == 0
            and args[1].shape[0] % 16 == 0
        )
        if owner_plan:
            return local_owner(sp_size, *args)
        return local_general(*args)

    return jax.shard_map(
        local, mesh=mesh, in_specs=placed, out_specs=P(("sp", "tp"), None), check_vma=False
    )
```
